32 devices in a mesh: sp: 16 (over z, y, x), tp: 2 (over core).
Axes of the slice: x: 2, y: 2, z: 4, core: 2. Of those that a mesh axis runs over, the one named last changes fastest.
Arguments:
- hidden_in: bfloat16 [4096, 2048], P('sp'), may hold values from -16 to 16
- query_one: bfloat16 [2048, 512], P(None, 'tp'), may hold values from -0.13258252 to 0.13258252
- query_two: bfloat16 [2048, 512], P(None, 'tp'), may hold values from -0.13258252 to 0.13258252
- key_one: bfloat16 [2048, 512], P(None, 'tp'), may hold values from -0.13258252 to 0.13258252
- key_two: bfloat16 [2048, 512], P(None, 'tp'), may hold values from -0.13258252 to 0.13258252
- value_proj: bfloat16 [2048, 1024], P(None, 'tp'), may hold values from -0.125 to 0.125
- lambdas: float32 [8], P('tp'), may hold values from 0.3 to 0.8
- norm_gain: float32 [128], replicated, may hold values from 0.1 to 1.9
- out_proj: bfloat16 [1024, 2048], P('tp'), may hold values from -0.1875 to 0.1875
Outputs:
- attended: bfloat16 [4096, 2048], P('sp')
The draws below stay inside these ranges and needn't reach their ends.
All inputs are finite; a program needn't handle non-finite values.
Results may differ from the reference program's by a relative error of at most 0.015.
Values may be sent and summed in bfloat16 or wider, within the bound.
No kernel may reach another device: no remote copies, remote signals or barrier semaphores. Data moves between devices by JAX's collectives and lax.ppermute only.
A program may use at most 64 MiB of HBM per device.

```python
import math
import jax
import jax.numpy as jnp
from jax import lax

D = 2048
HEADS = 8
HEAD_QK = 64
HEAD_V = 128
TOK_DEV = 256
TOKENS = 4096
N_TP = 2


def draw_hidden_in(key, part):
    blocks = TOKENS // TOK_DEV
    noise_key = jax.random.fold_in(key, 101)
    shift_key = jax.random.fold_in(key, 102)
    offsets = 0.6 * jax.random.normal(shift_key, (blocks, 1, D), jnp.float32)
    base = 0.8 * jax.random.normal(noise_key, (blocks, TOK_DEV, D), jnp.float32)
    field = base + offsets
    return jnp.clip(field.reshape(TOKENS, D), -16.0, 16.0).astype(jnp.bfloat16)


def plain_weight(key, salt):
    base = jax.random.normal(jax.random.fold_in(key, salt), (D, HEADS * HEAD_QK), jnp.float32)
    return jnp.clip(base, -6.0, 6.0) * D ** (-0.5)


def draw_query_one(key, part):
    return plain_weight(key, 201).astype(jnp.bfloat16)


def draw_query_two(key, part):
    return plain_weight(key, 301).astype(jnp.bfloat16)


def draw_key_one(key, part):
    return plain_weight(key, 211).astype(jnp.bfloat16)


def draw_key_two(key, part):
    return plain_weight(key, 311).astype(jnp.bfloat16)


def shard_levels(rng, dims, split, least, high):
    loudness = 1.0
    for dim, blocks in split:
        draws = jax.random.uniform(jax.random.fold_in(jax.random.fold_in(rng, 6), dim), (blocks,), jnp.float32, least / len(split), high / len(split))
        loudness = loudness * jnp.repeat(jnp.exp(draws), dims[dim] // blocks).reshape((-1,) + (1,) * (len(dims) - 1 - dim))
    return loudness


def scatter_about(key, dims, spread, bound, split=(), held_as=jnp.bfloat16):
    array = jax.random.normal(key, dims, jnp.float32) * spread
    if len(split) > 0:
        array = shard_levels(key, dims, split, -0.22, 0.18) * array
    return jnp.clip(array, min=-bound, max=bound).astype(held_as)


def setup_inputs(seed: int = 0) -> dict:
    key_list = jax.random.split(jax.random.key(seed), 10)
    hidden_in = draw_hidden_in(jax.random.fold_in(key_list[9], 71), 0)
    query_one = draw_query_one(jax.random.fold_in(key_list[9], 71), 0)
    query_two = draw_query_two(jax.random.fold_in(key_list[9], 71), 0)
    key_one = draw_key_one(jax.random.fold_in(key_list[9], 71), 0)
    key_two = draw_key_two(jax.random.fold_in(key_list[9], 71), 0)
    value_proj = scatter_about(key_list[5], (D, HEADS * HEAD_V), D ** -0.5, 0.125, ((1, 2),))
    lambdas = jnp.clip(0.3 + 0.5 * jax.random.uniform(key_list[6], (HEADS,), jnp.float32) ** shard_levels(key_list[6], (HEADS,), ((0, 2),), -0.2, 0.2), 0.3, 0.8)
    norm_gain = jnp.clip(1.0 + 0.18 * jax.random.normal(key_list[7], (HEAD_V,), jnp.float32), 0.1, 1.9)
    out_proj = scatter_about(key_list[8], (HEADS * HEAD_V, D), (HEADS * HEAD_V) ** -0.5, 0.1875, ((0, 2),))
    return {"hidden_in": hidden_in, "query_one": query_one, "query_two": query_two, "key_one": key_one, "key_two": key_two, "value_proj": value_proj, "lambdas": lambdas, "norm_gain": norm_gain, "out_proj": out_proj}


epsilon = 1e-06
masked_score = -1e+30

def reference(hidden_in, query_one, query_two, key_one, key_two, value_proj, lambdas, norm_gain, out_proj):

    def project(weight, width):
        product = jnp.dot(hidden_in, weight, preferred_element_type=jnp.float32)
        return product.astype(jnp.bfloat16).reshape(TOKENS, HEADS, width)
    query_a = project(query_one, HEAD_QK)
    query_b = project(query_two, HEAD_QK)
    keys_a = project(key_one, HEAD_QK).astype(jnp.float32)
    keys_b = project(key_two, HEAD_QK).astype(jnp.float32)
    value_rows = project(value_proj, HEAD_V).astype(jnp.float32)
    score_scale = 1.75 * HEAD_QK ** (-0.5)
    key_pos = jnp.arange(TOKENS, dtype=jnp.int32)
    query_rows = math.gcd(TOKENS, 512)

    def one_block(block_index):
        begin = block_index * query_rows
        row_pos = begin + jnp.arange(query_rows, dtype=jnp.int32)
        allowed = key_pos[None, :] <= row_pos[:, None]

        def attend(queries, keys):
            chosen = lax.dynamic_slice_in_dim(queries, begin, query_rows, 0).astype(jnp.float32)
            scores = jnp.einsum('qhd,khd->hqk', chosen, keys) * score_scale
            scores = jnp.where(allowed[None], scores, masked_score)
            highest = lax.optimization_barrier(jnp.max(scores, axis=-1, keepdims=True))
            expos = jnp.where(allowed[None], jnp.exp(scores - highest), 0.0)
            summed = lax.optimization_barrier(jnp.sum(expos, axis=-1))
            rounded = lax.optimization_barrier(expos.astype(jnp.bfloat16))
            accum = jnp.einsum('hqk,khe->hqe', rounded.astype(jnp.float32), value_rows)
            return accum / summed[..., None]
        mixed_out = attend(query_a, keys_a) - lambdas[:, None, None] * attend(query_b, keys_b)
        scale_rows = lax.rsqrt(lax.optimization_barrier(jnp.mean(mixed_out * mixed_out, axis=-1, keepdims=True)) + epsilon)
        normed = (mixed_out * scale_rows * norm_gain).astype(jnp.bfloat16)
        return jnp.transpose(normed, (1, 0, 2)).reshape(query_rows, HEADS * HEAD_V)
    normed = lax.map(one_block, jnp.arange(TOKENS // query_rows, dtype=jnp.int32))
    normed = normed.reshape(TOKENS, HEADS * HEAD_V)
    group_cols = HEADS * HEAD_V // N_TP
    summed = jnp.zeros((TOKENS, D), jnp.float32)
    for group_index in range(N_TP):
        lower = group_index * group_cols
        part = jnp.dot(normed[:, lower:lower + group_cols], out_proj[lower:lower + group_cols], preferred_element_type=jnp.float32).astype(jnp.bfloat16)
        part = lax.optimization_barrier(part)
        summed = summed + part.astype(jnp.float32)
    return summed.astype(jnp.bfloat16)
```

```python
import functools
import math

import jax
import jax.numpy as jnp
from jax import lax
from jax.experimental import pallas as pl
from jax.experimental.pallas import tpu as pltpu
from jax.sharding import PartitionSpec as P

epsilon = 1e-06
masked_score = -1e30
log2_e = 1.4426950408889634
least_sum = 2.0**-90
most_sum = 2.0**100
lanes = 128
both = ("sp", "tp")


def cost(flops, moved, transcendentals=0):
    return pl.CostEstimate(
        flops=int(flops), bytes_accessed=int(moved), transcendentals=int(transcendentals)
    )


def in_vmem():
    return pl.BlockSpec(memory_space=pltpu.VMEM)


def in_smem():
    return pl.BlockSpec(memory_space=pltpu.SMEM)


def anywhere():
    return pl.BlockSpec(memory_space=pl.ANY)


def pair_up(first, second, heads):
    tiles = []
    low = lax.broadcasted_iota(jnp.int32, (first.shape[0], lanes), 1) < lanes // 2
    for pair in range(heads // 2):
        columns = slice(pair * lanes, (pair + 1) * lanes)
        rolled = pltpu.roll(second[:, columns], lanes // 2, 1)
        tiles.append(jnp.where(low, first[:, columns], rolled))
        tiles.append(jnp.where(low, rolled, first[:, columns]))
    return tiles


def key_value_kernel(heads, place, hidden, key_one, key_two, value_proj, *refs):
    outs, stage = refs[:heads], refs[heads]
    rows = hidden.shape[0]
    tokens = hidden[...]
    first = jnp.dot(tokens, key_one[...], preferred_element_type=jnp.float32)
    second = jnp.dot(tokens, key_two[...], preferred_element_type=jnp.float32)
    for head, tile in enumerate(pair_up(first, second, heads)):
        stage[head, :rows, :] = tile.astype(jnp.bfloat16)
    values = jnp.dot(tokens, value_proj[...], preferred_element_type=jnp.float32)
    for head in range(heads):
        turned = values[:, head * lanes : (head + 1) * lanes].T.astype(jnp.bfloat16)
        for part in range(rows // lanes):
            at = rows + part * lanes
            stage[head, at : at + lanes, :] = turned[:, part * lanes : (part + 1) * lanes]
    for turn in range(heads):
        outs[turn][...] = stage[lax.rem(place[0] + turn, heads)]


def query_kernel(heads, scale, place, hidden, query_one, query_two, *refs):
    outs, stage = refs[:heads], refs[heads]
    tokens = hidden[...]
    first = jnp.dot(tokens, query_one[...], preferred_element_type=jnp.float32)
    second = jnp.dot(tokens, query_two[...], preferred_element_type=jnp.float32)
    for head, tile in enumerate(pair_up(first, second, heads)):
        stage[head] = (tile * scale).astype(jnp.bfloat16)
    for turn in range(heads):
        outs[turn][...] = stage[lax.rem(place[0] + turn, heads)]


def attend_kernel(heads, groups, across, place, lam_mine, lam_other, gain, *refs):
    z, y, x, t = place[0], place[1], place[2], place[3]
    parts = groups * across
    query_in = refs[:heads]
    block_in = refs[heads : heads + heads * parts]
    outs = refs[heads + heads * parts : 2 * heads + heads * parts]
    queries, blocks, accum, sums, peak, done, flag, sems = refs[2 * heads + heads * parts :]
    rows = queries.shape[1]
    head_v = lanes

    copies = []
    for turn in range(heads):
        source = lax.rem(z + heads - turn, heads)
        copies.append(
            pltpu.make_async_copy(query_in[turn], queries.at[source], sems.at[len(copies)])
        )
    for group in range(groups):
        for side in range(across):
            for turn in range(heads):
                source = lax.rem(z + heads - turn, heads)
                block = (source * groups + lax.rem(t + group, groups)) * across
                block = block + lax.rem(x + side, across)
                index = (group * across + side) * heads + turn
                copies.append(
                    pltpu.make_async_copy(block_in[index], blocks.at[block], sems.at[len(copies)])
                )
    for copy in copies:
        copy.start()
    for copy in copies:
        copy.wait()

    mine = t * across + x
    odd = lax.rem(z, 2) == 1
    lam = jnp.where(y == t, lam_mine[z], lam_other[z])
    weight_low = jnp.where(odd, -lam, 1.0)
    weight_high = jnp.where(odd, 1.0, -lam)
    lane = lax.broadcasted_iota(jnp.int32, (1, lanes), 1)
    low = jnp.where(lane < lanes // 2, 1.0, 0.0).astype(jnp.bfloat16)
    high = jnp.where(lane < lanes // 2, 0.0, 1.0).astype(jnp.bfloat16)
    width = 2 * rows
    key_row = lax.broadcasted_iota(jnp.int32, (rows, width), 0)
    query_col = lax.broadcasted_iota(jnp.int32, (rows, width), 1)
    ahead = key_row - jnp.where(query_col < rows, query_col, query_col - rows)

    def scores_of(block, two_maps):
        return lax.dot_general(
            blocks[block, :rows, :],
            two_maps,
            (((1,), (1,)), ((), ())),
            preferred_element_type=jnp.float32,
        )

    def values_of(block):
        pieces = [
            blocks[block, rows + p * lanes : rows + (p + 1) * lanes, :]
            for p in range(rows // lanes)
        ]
        return jnp.concatenate(pieces, axis=1)

    def fold(weights):
        return jnp.sum(weights.reshape(rows // 8, 8, width), axis=0)

    def stripe(first, two_maps, masked):
        added = jnp.zeros((head_v, width), jnp.float32)
        total = jnp.zeros((8, width), jnp.float32)
        for part in range(parts):
            block = first + part
            weights = jnp.exp2(scores_of(block, two_maps))
            if masked:
                weights = jnp.where(ahead <= (mine - part) * rows, weights, 0.0)
            total = total + fold(weights)
            added = added + jnp.dot(
                values_of(block),
                weights.astype(jnp.bfloat16),
                preferred_element_type=jnp.float32,
            )
        return added, total

    def finish(index):
        total = jnp.sum(sums[...], axis=0, keepdims=True)
        heads_out = accum[...] * (1.0 / total)
        mixed = heads_out[:, :rows] * weight_low + heads_out[:, rows:] * weight_high
        scale = lax.rsqrt(jnp.mean(mixed * mixed, axis=0, keepdims=True) + epsilon)
        done[index] = ((mixed * scale).T * gain[...]).astype(jnp.bfloat16)
        return total

    def two_maps_of(index):
        chosen = queries[index]
        return jnp.concatenate([chosen * low, chosen * high], axis=0)

    flag[...] = jnp.zeros_like(flag)

    def one_stripe(index, carried):
        two_maps = two_maps_of(index)
        added, total = stripe(index * parts, two_maps, True)
        accum[...] = added
        sums[...] = total

        def earlier(before, inner):
            more, weight = stripe(before * parts, two_maps, False)
            accum[...] += more
            sums[...] += weight
            return inner

        lax.fori_loop(0, index, earlier, 0)
        total = finish(index)
        inside = (total >= least_sum) & (total <= most_sum)
        flag[...] = jnp.maximum(flag[...], jnp.where(inside, 0.0, 1.0))
        return carried

    lax.fori_loop(0, heads, one_stripe, 0)

    @pl.when(jnp.max(flag[...]) > 0.0)
    def _():
        def redo(index, carried):
            two_maps = two_maps_of(index)
            accum[...] = jnp.zeros_like(accum)
            sums[...] = jnp.zeros_like(sums)
            peak[...] = jnp.full(peak.shape, masked_score, jnp.float32)

            def one_block(block, inner):
                allowed = ahead <= (index * parts + mine - block) * rows
                scores = jnp.where(allowed, scores_of(block, two_maps), masked_score)
                highest = jnp.maximum(peak[...], jnp.max(scores, axis=0, keepdims=True))
                rescale = jnp.exp2(peak[...] - highest)
                weights = jnp.where(allowed, jnp.exp2(scores - highest), 0.0)
                sums[...] = sums[...] * rescale + fold(weights)
                accum[...] = accum[...] * rescale + jnp.dot(
                    values_of(block),
                    weights.astype(jnp.bfloat16),
                    preferred_element_type=jnp.float32,
                )
                peak[...] = highest
                return inner

            lax.fori_loop(0, index * parts + mine + 1, one_block, 0)
            finish(index)
            return carried

        lax.fori_loop(0, heads, redo, 0)

    for turn in range(heads):
        outs[turn][...] = done[lax.rem(z + heads - turn, heads)]


def project_out_kernel(heads, place, *refs):
    mine, other = refs[:heads], refs[heads : 2 * heads]
    out_mine, out_other, result, joined = refs[2 * heads :]
    z = place[0]
    for turn in range(heads):
        at = pl.multiple_of(lax.rem(z + turn, heads) * lanes, lanes)
        joined[0, :, pl.ds(at, lanes)] = mine[turn][...]
        joined[1, :, pl.ds(at, lanes)] = other[turn][...]
    total = jnp.dot(joined[0], out_mine[...], preferred_element_type=jnp.float32)
    total = total + jnp.dot(joined[1], out_other[...], preferred_element_type=jnp.float32)
    result[...] = total.astype(jnp.bfloat16)


def exchanged(
    hidden_in, query_one, query_two, key_one, key_two, value_proj, lambdas, norm_gain, out_proj
):
    heads = lambdas.shape[0]
    groups = lax.axis_size("tp")
    across = lax.axis_size("sp") // (heads * groups)
    parts = groups * across
    rows, model = hidden_in.shape
    head_qk = query_one.shape[1] // heads
    scale = 1.75 * head_qk ** (-0.5) * log2_e
    bf16 = jnp.bfloat16

    sp_index = lax.axis_index("sp")
    z = sp_index // parts
    y = (sp_index // across) % groups
    x = sp_index % across
    t = lax.axis_index("tp")
    place = jnp.stack([z, y, x, t]).astype(jnp.int32)

    def line(zz, yy, xx, cc):
        return ((zz * groups + yy) * across + xx) * groups + cc

    def round_of(turn):
        pairs = []
        for zz in range(heads):
            for yy in range(groups):
                for xx in range(across):
                    for cc in range(groups):
                        pairs.append(
                            (line(zz, yy, xx, cc), line((zz + turn) % heads, cc, xx, yy))
                        )
        return pairs

    swap_core = [(i, (i + 1) % groups) for i in range(groups)]
    swap_side = [(i, i - i % across + (i + 1) % across) for i in range(heads * parts)]

    lam_other = lax.ppermute(lambdas, "tp", swap_core)
    out_other = lax.ppermute(out_proj, "tp", swap_core)

    block_rows = 2 * rows
    kv = pl.pallas_call(
        functools.partial(key_value_kernel, heads),
        out_shape=[jax.ShapeDtypeStruct((block_rows, lanes), bf16)] * heads,
        in_specs=[in_smem()] + [in_vmem()] * 4,
        out_specs=[in_vmem()] * heads,
        scratch_shapes=[pltpu.VMEM((heads, block_rows, lanes), bf16)],
        compiler_params=pltpu.CompilerParams(vmem_limit_bytes=24 << 20),
        cost_estimate=cost(2 * rows * model * 4 * heads * head_qk, 6 << 20),
        name="project_keys",
    )(place, hidden_in, key_one, key_two, value_proj)
    queries = pl.pallas_call(
        functools.partial(query_kernel, heads, scale),
        out_shape=[jax.ShapeDtypeStruct((rows, lanes), bf16)] * heads,
        in_specs=[in_smem()] + [in_vmem()] * 3,
        out_specs=[in_vmem()] * heads,
        scratch_shapes=[pltpu.VMEM((heads, rows, lanes), bf16)],
        compiler_params=pltpu.CompilerParams(vmem_limit_bytes=24 << 20),
        cost_estimate=cost(2 * rows * model * 2 * heads * head_qk, 4 << 20),
        name="project_queries",
    )(place, hidden_in, query_one, query_two)

    own = [lax.ppermute(kv[turn], both, round_of(turn)) for turn in range(heads)]
    moved_queries = [lax.ppermute(queries[turn], both, round_of(turn)) for turn in range(heads)]
    beside = [lax.ppermute(block, "sp", swap_side) for block in own]
    own_swapped = [lax.ppermute(block, "tp", swap_core) for block in own]
    beside_swapped = [lax.ppermute(block, "tp", swap_core) for block in beside]
    blocks = own + beside + own_swapped + beside_swapped

    tokens = heads * rows
    normed = pl.pallas_call(
        functools.partial(attend_kernel, heads, groups, across),
        out_shape=[jax.ShapeDtypeStruct((rows, lanes), bf16)] * heads,
        in_specs=[in_smem()] * 3 + [in_vmem()] + [anywhere()] * (heads + heads * parts),
        out_specs=[in_vmem()] * heads,
        scratch_shapes=[
            pltpu.VMEM((heads, rows, lanes), bf16),
            pltpu.VMEM((heads * parts, block_rows, lanes), bf16),
            pltpu.VMEM((lanes, 2 * rows), jnp.float32),
            pltpu.VMEM((8, 2 * rows), jnp.float32),
            pltpu.VMEM((1, 2 * rows), jnp.float32),
            pltpu.VMEM((heads, rows, lanes), bf16),
            pltpu.VMEM((1, 2 * rows), jnp.float32),
            pltpu.SemaphoreType.DMA((heads + heads * parts,)),
        ],
        compiler_params=pltpu.CompilerParams(vmem_limit_bytes=32 << 20),
        cost_estimate=cost(2 * 2 * tokens * tokens * parts * lanes, 3 << 20),
        name="attend",
    )(place, lambdas, lam_other, norm_gain.reshape(1, lanes), *queries_in(moved_queries), *blocks)

    back = []
    for turn in range(heads):
        back.append(lax.ppermute(normed[turn], both, [(b, a) for a, b in round_of(turn)]))
    back_other = [lax.ppermute(piece, "tp", swap_core) for piece in back]
    return pl.pallas_call(
        functools.partial(project_out_kernel, heads),
        out_shape=jax.ShapeDtypeStruct((rows, model), bf16),
        in_specs=[in_smem()] + [in_vmem()] * (2 * heads + 2),
        out_specs=in_vmem(),
        scratch_shapes=[pltpu.VMEM((groups, rows, heads * lanes), bf16)],
        compiler_params=pltpu.CompilerParams(vmem_limit_bytes=24 << 20),
        cost_estimate=cost(2 * rows * model * groups * heads * lanes, 6 << 20),
        name="project_out",
    )(place, *back, *back_other, out_proj, out_other)


def queries_in(arrays):
    return tuple(arrays)


def gathered(
    hidden_in, query_one, query_two, key_one, key_two, value_proj, lambdas, norm_gain, out_proj
):
    heads_dev = lambdas.shape[0]
    head_qk = query_one.shape[1] // heads_dev
    head_v = value_proj.shape[1] // heads_dev
    width_q = heads_dev * head_qk
    score_scale = 1.75 * head_qk ** (-0.5)
    joined = jnp.concatenate((query_one, query_two, key_one, key_two, value_proj), axis=1)
    projected = jnp.dot(hidden_in, joined, preferred_element_type=jnp.float32).astype(jnp.bfloat16)
    tok_rows = projected.shape[0]
    key_values = projected[:, 2 * width_q :]
    my_index = lax.axis_index("sp")
    positions = my_index * tok_rows + jnp.arange(tok_rows, dtype=jnp.int32)
    query_a = projected[:, :width_q].reshape(tok_rows, heads_dev, head_qk)
    query_b = projected[:, width_q : 2 * width_q].reshape(tok_rows, heads_dev, head_qk)
    last_pos = positions[tok_rows - 1]

    def one_map(queries, keys, value_rows, allowed, running_max, running_sum, accum):
        scores = (
            jnp.einsum("qhd,khd->hqk", queries, keys, preferred_element_type=jnp.float32)
            * score_scale
        )
        scores = jnp.where(allowed[None], scores, masked_score)
        new_max = jnp.maximum(running_max, jnp.max(scores, axis=-1))
        rescale = jnp.exp(running_max - new_max)
        weights = jnp.where(allowed[None], jnp.exp(scores - new_max[..., None]), 0.0)
        new_sum = running_sum * rescale + jnp.sum(weights, axis=-1)
        added = jnp.einsum(
            "hqk,khe->hqe",
            weights.astype(jnp.bfloat16),
            value_rows,
            preferred_element_type=jnp.float32,
        )
        return (new_max, new_sum, accum * rescale[..., None] + added)

    def absorb(state, kblock, kstart):
        block_rows = kblock.shape[0]
        k_pos = kstart + jnp.arange(block_rows, dtype=jnp.int32)
        allowed = k_pos[None, :] <= positions[:, None]
        keys_a = kblock[:, :width_q].reshape(block_rows, heads_dev, head_qk)
        keys_b = kblock[:, width_q : 2 * width_q].reshape(block_rows, heads_dev, head_qk)
        value_rows = kblock[:, 2 * width_q :].reshape(block_rows, heads_dev, head_v)
        first_map = one_map(query_a, keys_a, value_rows, allowed, *state[:3])
        second_map = one_map(query_b, keys_b, value_rows, allowed, *state[3:])
        return first_map + second_map

    start_max = jnp.full((heads_dev, tok_rows), masked_score, jnp.float32)
    start_sum = jnp.zeros((heads_dev, tok_rows), jnp.float32)
    start_acc = jnp.zeros((heads_dev, tok_rows, head_v), jnp.float32)
    state = (start_max, start_sum, start_acc, start_max, start_sum, start_acc)
    kv_piece = lax.all_gather(key_values, "sp", axis=0, tiled=True)
    piece_rows = kv_piece.shape[0]
    block_rows = math.gcd(piece_rows, 512)
    block_count = piece_rows // block_rows
    stacked = kv_piece.reshape(block_count, block_rows, kv_piece.shape[1])

    def absorb_step(carried, blocks_in):
        kblock, block_index = blocks_in
        kstart = block_index * block_rows
        renewed = lax.cond(
            kstart <= last_pos,
            lambda inner: absorb(inner, kblock, kstart),
            lambda inner: inner,
            carried,
        )
        return (renewed, None)

    state, _ = lax.scan(absorb_step, state, (stacked, jnp.arange(block_count, dtype=jnp.int32)))
    out_a = state[2] / state[1][..., None]
    out_b = state[5] / state[4][..., None]
    mixed_out = out_a - lambdas[:, None, None] * out_b
    scale_rows = lax.rsqrt(jnp.mean(mixed_out * mixed_out, axis=-1, keepdims=True) + epsilon)
    normed = (mixed_out * scale_rows * norm_gain).astype(jnp.bfloat16)
    normed_all = jnp.transpose(normed, (1, 0, 2)).reshape(tok_rows, heads_dev * head_v)
    partial_value = jnp.dot(normed_all, out_proj, preferred_element_type=jnp.float32)
    return lax.psum(partial_value.astype(jnp.bfloat16), "tp")


def shards(*args):
    hidden_in, query_one, value_proj, lambdas = args[0], args[1], args[5], args[6]
    heads = lambdas.shape[0]
    groups, length = lax.axis_size("tp"), lax.axis_size("sp")
    fits = (
        groups == 2
        and heads % 2 == 0
        and length == 2 * groups * heads
        and query_one.shape[1] == heads * (lanes // 2)
        and value_proj.shape[1] == heads * lanes
        and hidden_in.shape[0] % lanes == 0
        and hidden_in.shape[0] <= 512
    )
    return exchanged(*args) if fits else gathered(*args)


def solution(mesh):
    placed = (
        P("sp", None),
        P(None, "tp"),
        P(None, "tp"),
        P(None, "tp"),
        P(None, "tp"),
        P(None, "tp"),
        P("tp"),
        P(),
        P("tp", None),
    )
    return jax.shard_map(
        shards, mesh=mesh, in_specs=placed, out_specs=P("sp", None), check_vma=False
    )
```

```python
import functools
import math

import jax
import jax.numpy as jnp
from jax import lax
from jax.experimental import pallas as pl
from jax.experimental.pallas import tpu as pltpu
from jax.sharding import PartitionSpec as P


epsilon = 1e-06
masked_score = -1e30
log2_e = 1.4426950408889634
least_sum = 2.0**-90
most_sum = 2.0**100
lanes = 128


def cost(flops, moved):
    return pl.CostEstimate(flops=int(flops), bytes_accessed=int(moved), transcendentals=0)


def in_vmem():
    return pl.BlockSpec(memory_space=pltpu.VMEM)


def in_smem():
    return pl.BlockSpec(memory_space=pltpu.SMEM)


def in_hbm():
    return pl.BlockSpec(memory_space=pltpu.HBM)


def pair_up(first, second, heads):
    tiles = []
    low = lax.broadcasted_iota(jnp.int32, (first.shape[0], lanes), 1) < lanes // 2
    for pair in range(heads // 2):
        columns = slice(pair * lanes, (pair + 1) * lanes)
        rolled = pltpu.roll(second[:, columns], lanes // 2, 1)
        tiles.append(jnp.where(low, first[:, columns], rolled))
        tiles.append(jnp.where(low, rolled, first[:, columns]))
    return tiles


def fetch(arrays, buffers, sems):
    copies = []
    for index, (array, buffer) in enumerate(zip(arrays, buffers)):
        copies.append(pltpu.make_async_copy(array, buffer, sems.at[index]))
    for copy in copies:
        copy.start()
    return copies


def turned_into(stage, head, at, tile):
    turned = tile.T.astype(jnp.bfloat16)
    for part in range(tile.shape[0] // lanes):
        begin = at + part * lanes
        stage[head, begin : begin + lanes, :] = turned[:, part * lanes : (part + 1) * lanes]


def key_value_kernel(heads, place, *refs):
    arrays, outs = refs[:6], refs[6 : 6 + heads]
    hidden, query_one, query_two = refs[6 + heads : 9 + heads]
    key_one, key_two, value_proj, stage, sems = refs[9 + heads :]
    buffers = (hidden, key_one, key_two, value_proj, query_one, query_two)
    copies = fetch(arrays, buffers, sems)
    rows = hidden.shape[0]
    copies[0].wait()
    copies[1].wait()
    first = jnp.dot(hidden[...], key_one[...], preferred_element_type=jnp.float32)
    copies[2].wait()
    second = jnp.dot(hidden[...], key_two[...], preferred_element_type=jnp.float32)
    for head, tile in enumerate(pair_up(first, second, heads)):
        stage[head, :rows, :] = tile.astype(jnp.bfloat16)
    copies[3].wait()
    values = jnp.dot(hidden[...], value_proj[...], preferred_element_type=jnp.float32)
    for head in range(heads):
        turned_into(stage, head, rows, values[:, head * lanes : (head + 1) * lanes])
    for turn in range(heads):
        outs[turn][...] = stage[place[0] ^ turn]
    copies[4].wait()
    copies[5].wait()


def query_kernel(heads, scale, place, hidden, query_one, query_two, *refs):
    outs, stage = refs[:heads], refs[heads]
    first = jnp.dot(hidden[...], query_one[...], preferred_element_type=jnp.float32)
    second = jnp.dot(hidden[...], query_two[...], preferred_element_type=jnp.float32)
    for head, tile in enumerate(pair_up(first, second, heads)):
        turned_into(stage, head, 0, tile * scale)
    for turn in range(heads):
        outs[turn][...] = stage[place[0] ^ turn]


def attend_kernel(heads, down, across, place, lambdas, gain, *refs):
    z, y, x = place[0], place[1], place[2]
    parts = down * across
    query_in, refs = refs[:heads], refs[heads:]
    block_in, refs = refs[: heads * parts], refs[heads * parts :]
    outs, refs = refs[:heads], refs[heads:]
    queries, keys, values, accum, sums, peak, done, flag = refs
    rows = queries.shape[1]
    width = 2 * rows
    span = parts * rows
    bf16 = jnp.bfloat16

    for turn in range(heads):
        queries[z ^ turn] = query_in[turn][...]
    for below in range(down):
        for aside in range(across):
            for turn in range(heads):
                block = ((z ^ turn) * down + (y ^ below)) * across + (x ^ aside)
                given = block_in[(below * across + aside) * heads + turn]
                at = pl.multiple_of(block * rows, rows)
                keys[pl.ds(at, rows), :] = given[:rows, :]
                for part in range(rows // lanes):
                    begin = rows + part * lanes
                    column = pl.multiple_of(at + part * lanes, lanes)
                    values[:, pl.ds(column, lanes)] = given[begin : begin + lanes, :]

    mine = y * across + x
    odd = lax.rem(z, 2) == 1
    lam = lambdas[z]
    weight_low = jnp.where(odd, -lam, 1.0)
    weight_high = jnp.where(odd, 1.0, -lam)

    def ahead_of(count):
        key_row = lax.broadcasted_iota(jnp.int32, (count, width), 0)
        query_col = lax.broadcasted_iota(jnp.int32, (count, width), 1)
        return key_row - jnp.where(query_col < rows, query_col, query_col - rows)

    def two_maps_of(index):
        pieces = [
            queries[index, part * lanes : (part + 1) * lanes, :] for part in range(rows // lanes)
        ]
        joined = jnp.concatenate(pieces, axis=1)
        nothing = jnp.zeros((lanes // 2, rows), bf16)
        low = jnp.concatenate([joined[: lanes // 2], nothing], axis=0)
        high = jnp.concatenate([nothing, joined[lanes // 2 :]], axis=0)
        return jnp.concatenate([low, high], axis=1)

    def scores_of(at, count, two_maps):
        return jnp.dot(keys[pl.ds(at, count), :], two_maps, preferred_element_type=jnp.float32)

    def weighed(at, count, weights):
        return jnp.dot(
            values[:, pl.ds(at, count)], weights.astype(bf16), preferred_element_type=jnp.float32
        )

    def fold(weights):
        return jnp.sum(weights.reshape(weights.shape[0] // 8, 8, width), axis=0)

    def finish(index, added, total):
        total = jnp.sum(total, axis=0, keepdims=True)
        heads_out = added * (1.0 / total)
        mixed = heads_out[:, :rows] * weight_low + heads_out[:, rows:] * weight_high
        scale = lax.rsqrt(jnp.mean(mixed * mixed, axis=0, keepdims=True) + epsilon)
        done[index] = ((mixed * scale).T * gain[...]).astype(bf16)
        return total

    flag[...] = jnp.zeros_like(flag)
    for index in range(heads):
        two_maps = two_maps_of(index)
        weights = jnp.exp2(scores_of(index * span, span, two_maps))
        weights = jnp.where(ahead_of(span) <= mine * rows, weights, 0.0)
        total = fold(weights)
        added = weighed(index * span, span, weights)
        for before in range(index):
            weights = jnp.exp2(scores_of(before * span, span, two_maps))
            total = total + fold(weights)
            added = added + weighed(before * span, span, weights)
        total = finish(index, added, total)
        inside = (total >= least_sum) & (total <= most_sum)
        flag[...] = jnp.maximum(flag[...], jnp.where(inside, 0.0, 1.0))

    @pl.when(jnp.max(flag[...]) > 0.0)
    def _():
        def redo(index, carried):
            two_maps = two_maps_of(index)
            accum[...] = jnp.zeros_like(accum)
            sums[...] = jnp.zeros_like(sums)
            peak[...] = jnp.full(peak.shape, masked_score, jnp.float32)

            def one_block(block, inner):
                at = pl.multiple_of(block * rows, rows)
                allowed = ahead_of(rows) <= (index * parts + mine - block) * rows
                scores = jnp.where(allowed, scores_of(at, rows, two_maps), masked_score)
                highest = jnp.maximum(peak[...], jnp.max(scores, axis=0, keepdims=True))
                rescale = jnp.exp2(peak[...] - highest)
                weights = jnp.where(allowed, jnp.exp2(scores - highest), 0.0)
                sums[...] = sums[...] * rescale + fold(weights)
                accum[...] = accum[...] * rescale + weighed(at, rows, weights)
                peak[...] = highest
                return inner

            lax.fori_loop(0, index * parts + mine + 1, one_block, 0)
            finish(index, accum[...], sums[...])
            return carried

        lax.fori_loop(0, heads, redo, 0)

    for turn in range(heads):
        outs[turn][...] = done[z ^ turn]


def join_kernel(heads, place, *refs):
    pieces, joined = refs[:heads], refs[heads]
    for turn in range(heads):
        at = pl.multiple_of((place[0] ^ turn) * lanes, lanes)
        joined[:, pl.ds(at, lanes)] = pieces[turn][...]


def project_out_kernel(mine, other, out_mine, out_other, result, staged, sems):
    copies = []
    pieces = sems.shape[0]
    wide = result.shape[1] // pieces
    for piece in range(pieces):
        columns = slice(piece * wide, (piece + 1) * wide)
        total = jnp.dot(mine[...], out_mine[:, columns], preferred_element_type=jnp.float32)
        total = total + jnp.dot(
            other[...], out_other[:, columns], preferred_element_type=jnp.float32
        )
        staged[:, columns] = total.astype(jnp.bfloat16)
        copies.append(
            pltpu.make_async_copy(staged.at[:, columns], result.at[:, columns], sems.at[piece])
        )
        copies[-1].start()
    for copy in copies:
        copy.wait()


def from_hbm(*arrays):
    return [pltpu.with_memory_space_constraint(array, pltpu.HBM) for array in arrays]


def exchanged(
    hidden_in, query_one, query_two, key_one, key_two, value_proj, lambdas, norm_gain, out_proj
):
    heads = lambdas.shape[0]
    groups = lax.axis_size("tp")
    down = across = 2
    parts = down * across
    rows, model = hidden_in.shape
    head_qk = query_one.shape[1] // heads
    width = heads * head_qk
    scale = 1.75 * head_qk ** (-0.5) * log2_e
    bf16 = jnp.bfloat16
    f32 = jnp.float32

    sp_index = lax.axis_index("sp")
    z = sp_index // parts
    y = (sp_index // across) % down
    x = sp_index % across
    place = jnp.stack([z, y, x]).astype(jnp.int32)

    def exchange(array, step):
        pairs = [(index, index ^ step) for index in range(heads * parts)]
        return lax.ppermute(array, "sp", pairs)

    swap_core = [(i, (i + 1) % groups) for i in range(groups)]
    turns = range(heads)

    block_rows = 2 * rows
    block = jax.ShapeDtypeStruct((block_rows, lanes), bf16)
    stripe = jax.ShapeDtypeStruct((rows, lanes), bf16)
    fetched = (hidden_in, query_one, query_two)
    made = pl.pallas_call(
        functools.partial(key_value_kernel, heads),
        out_shape=[block] * heads + [jax.ShapeDtypeStruct(a.shape, bf16) for a in fetched],
        in_specs=[in_smem()] + [in_hbm()] * 6,
        out_specs=[in_vmem()] * (heads + 3),
        scratch_shapes=[
            pltpu.VMEM((model, width), bf16),
            pltpu.VMEM((model, width), bf16),
            pltpu.VMEM((model, heads * lanes), bf16),
            pltpu.VMEM((heads, block_rows, lanes), bf16),
            pltpu.SemaphoreType.DMA((6,)),
        ],
        compiler_params=pltpu.CompilerParams(vmem_limit_bytes=20 << 20),
        cost_estimate=cost(2 * rows * model * 4 * width, 7 << 20),
        name="project_keys",
    )(place, *from_hbm(hidden_in, key_one, key_two, value_proj, query_one, query_two))
    kv, held = made[:heads], made[heads:]
    own = [kv[0]] + [exchange(kv[turn], turn * parts) for turn in turns[1:]]

    queries = pl.pallas_call(
        functools.partial(query_kernel, heads, scale),
        out_shape=[stripe] * heads,
        in_specs=[in_smem()] + [in_vmem()] * 3,
        out_specs=[in_vmem()] * heads,
        scratch_shapes=[pltpu.VMEM((heads, rows, lanes), bf16)],
        compiler_params=pltpu.CompilerParams(vmem_limit_bytes=16 << 20),
        cost_estimate=cost(2 * rows * model * 2 * width, 4 << 20),
        name="project_queries",
    )(place, *held)
    own_queries = [queries[0]]
    for turn in turns[1:]:
        own_queries.append(exchange(queries[turn], turn * parts))

    out_other = lax.ppermute(out_proj, "tp", swap_core)
    aside = [exchange(own[turn], 1) for turn in turns]
    below = [exchange(own[turn], across) for turn in turns]
    corner = [exchange(own[turn], 1 + across) for turn in turns]
    blocks = own + aside + below + corner

    tokens = heads * rows
    normed = pl.pallas_call(
        functools.partial(attend_kernel, heads, down, across),
        out_shape=[jax.ShapeDtypeStruct((rows, lanes), bf16)] * heads,
        in_specs=[in_smem()] * 2 + [in_vmem()] * (1 + heads + heads * parts),
        out_specs=[in_vmem()] * heads,
        scratch_shapes=[
            pltpu.VMEM((heads, rows, lanes), bf16),
            pltpu.VMEM((parts * tokens, lanes), bf16),
            pltpu.VMEM((lanes, parts * tokens), bf16),
            pltpu.VMEM((lanes, 2 * rows), f32),
            pltpu.VMEM((8, 2 * rows), f32),
            pltpu.VMEM((1, 2 * rows), f32),
            pltpu.VMEM((heads, rows, lanes), bf16),
            pltpu.VMEM((1, 2 * rows), f32),
        ],
        compiler_params=pltpu.CompilerParams(vmem_limit_bytes=32 << 20),
        cost_estimate=cost(4 * tokens * tokens * parts * lanes, 3 << 20),
        name="attend",
    )(place, lambdas, norm_gain.reshape(1, lanes), *own_queries, *blocks)

    back = [normed[0]]
    for turn in turns[1:]:
        back.append(exchange(normed[turn], turn * parts))
    joined = pl.pallas_call(
        functools.partial(join_kernel, heads),
        out_shape=jax.ShapeDtypeStruct((rows, heads * lanes), bf16),
        in_specs=[in_smem()] + [in_vmem()] * heads,
        out_specs=in_vmem(),
        compiler_params=pltpu.CompilerParams(vmem_limit_bytes=4 << 20),
        cost_estimate=cost(0, 2 * rows * heads * lanes),
        name="join",
    )(place, *back)
    joined_other = lax.ppermute(joined, "tp", swap_core)
    return pl.pallas_call(
        project_out_kernel,
        out_shape=jax.ShapeDtypeStruct((rows, model), bf16),
        in_specs=[in_vmem()] * 4,
        out_specs=in_hbm(),
        scratch_shapes=[pltpu.VMEM((rows, model), bf16), pltpu.SemaphoreType.DMA((4,))],
        compiler_params=pltpu.CompilerParams(vmem_limit_bytes=16 << 20),
        cost_estimate=cost(2 * rows * model * groups * heads * lanes, 6 << 20),
        name="project_out",
    )(joined, joined_other, out_proj, out_other)


def gathered(
    hidden_in, query_one, query_two, key_one, key_two, value_proj, lambdas, norm_gain, out_proj
):
    heads_dev = lambdas.shape[0]
    head_qk = query_one.shape[1] // heads_dev
    head_v = value_proj.shape[1] // heads_dev
    width_q = heads_dev * head_qk
    score_scale = 1.75 * head_qk ** (-0.5)
    joined = jnp.concatenate((query_one, query_two, key_one, key_two, value_proj), axis=1)
    projected = jnp.dot(hidden_in, joined, preferred_element_type=jnp.float32).astype(jnp.bfloat16)
    tok_rows = projected.shape[0]
    key_values = projected[:, 2 * width_q :]
    my_index = lax.axis_index("sp")
    positions = my_index * tok_rows + jnp.arange(tok_rows, dtype=jnp.int32)
    query_a = projected[:, :width_q].reshape(tok_rows, heads_dev, head_qk)
    query_b = projected[:, width_q : 2 * width_q].reshape(tok_rows, heads_dev, head_qk)
    last_pos = positions[tok_rows - 1]

    def one_map(queries, keys, value_rows, allowed, running_max, running_sum, accum):
        scores = (
            jnp.einsum("qhd,khd->hqk", queries, keys, preferred_element_type=jnp.float32)
            * score_scale
        )
        scores = jnp.where(allowed[None], scores, masked_score)
        new_max = jnp.maximum(running_max, jnp.max(scores, axis=-1))
        rescale = jnp.exp(running_max - new_max)
        weights = jnp.where(allowed[None], jnp.exp(scores - new_max[..., None]), 0.0)
        new_sum = running_sum * rescale + jnp.sum(weights, axis=-1)
        added = jnp.einsum(
            "hqk,khe->hqe",
            weights.astype(jnp.bfloat16),
            value_rows,
            preferred_element_type=jnp.float32,
        )
        return (new_max, new_sum, accum * rescale[..., None] + added)

    def absorb(state, kblock, kstart):
        block_rows = kblock.shape[0]
        k_pos = kstart + jnp.arange(block_rows, dtype=jnp.int32)
        allowed = k_pos[None, :] <= positions[:, None]
        keys_a = kblock[:, :width_q].reshape(block_rows, heads_dev, head_qk)
        keys_b = kblock[:, width_q : 2 * width_q].reshape(block_rows, heads_dev, head_qk)
        value_rows = kblock[:, 2 * width_q :].reshape(block_rows, heads_dev, head_v)
        first_map = one_map(query_a, keys_a, value_rows, allowed, *state[:3])
        second_map = one_map(query_b, keys_b, value_rows, allowed, *state[3:])
        return first_map + second_map

    start_max = jnp.full((heads_dev, tok_rows), masked_score, jnp.float32)
    start_sum = jnp.zeros((heads_dev, tok_rows), jnp.float32)
    start_acc = jnp.zeros((heads_dev, tok_rows, head_v), jnp.float32)
    state = (start_max, start_sum, start_acc, start_max, start_sum, start_acc)
    kv_piece = lax.all_gather(key_values, "sp", axis=0, tiled=True)
    piece_rows = kv_piece.shape[0]
    block_rows = math.gcd(piece_rows, 512)
    block_count = piece_rows // block_rows
    stacked = kv_piece.reshape(block_count, block_rows, kv_piece.shape[1])

    def absorb_step(carried, blocks_in):
        kblock, block_index = blocks_in
        kstart = block_index * block_rows
        renewed = lax.cond(
            kstart <= last_pos,
            lambda inner: absorb(inner, kblock, kstart),
            lambda inner: inner,
            carried,
        )
        return (renewed, None)

    state, _ = lax.scan(absorb_step, state, (stacked, jnp.arange(block_count, dtype=jnp.int32)))
    out_a = state[2] / state[1][..., None]
    out_b = state[5] / state[4][..., None]
    mixed_out = out_a - lambdas[:, None, None] * out_b
    scale_rows = lax.rsqrt(jnp.mean(mixed_out * mixed_out, axis=-1, keepdims=True) + epsilon)
    normed = (mixed_out * scale_rows * norm_gain).astype(jnp.bfloat16)
    normed_all = jnp.transpose(normed, (1, 0, 2)).reshape(tok_rows, heads_dev * head_v)
    partial_value = jnp.dot(normed_all, out_proj, preferred_element_type=jnp.float32)
    return lax.psum(partial_value.astype(jnp.bfloat16), "tp")


def shards(*args):
    hidden_in, query_one, value_proj, lambdas = args[0], args[1], args[5], args[6]
    heads = lambdas.shape[0]
    groups, length = lax.axis_size("tp"), lax.axis_size("sp")
    fits = (
        groups == 2
        and heads == 4
        and length == 4 * heads
        and query_one.shape[1] == heads * (lanes // 2)
        and value_proj.shape[1] == heads * lanes
        and hidden_in.shape[0] % lanes == 0
        and hidden_in.shape[0] <= 512
    )
    if not fits:
        return gathered(*args)
    return exchanged(*args)


def solution(mesh):
    placed = (
        P("sp", None),
        P(None, "tp"),
        P(None, "tp"),
        P(None, "tp"),
        P(None, "tp"),
        P(None, "tp"),
        P("tp"),
        P(),
        P("tp", None),
    )
    return jax.shard_map(
        shards, mesh=mesh, in_specs=placed, out_specs=P("sp", None), check_vma=False
    )
```

```python
import functools
import math

import jax
import jax.numpy as jnp
from jax import lax
from jax.experimental import pallas as pl
from jax.experimental.pallas import tpu as pltpu
from jax.sharding import PartitionSpec as P


epsilon = 1e-06
masked_score = -1e30
log2_e = 1.4426950408889634
least_sum = 2.0**-90
most_sum = 2.0**100
lanes = 128


def cost(flops, moved):
    return pl.CostEstimate(flops=int(flops), bytes_accessed=int(moved), transcendentals=0)


def in_vmem():
    return pl.BlockSpec(memory_space=pltpu.VMEM)


def in_smem():
    return pl.BlockSpec(memory_space=pltpu.SMEM)


def in_hbm():
    return pl.BlockSpec(memory_space=pltpu.HBM)


def pair_up(first, second, heads):
    tiles = []
    low = lax.broadcasted_iota(jnp.int32, (first.shape[0], lanes), 1) < lanes // 2
    for pair in range(heads // 2):
        columns = slice(pair * lanes, (pair + 1) * lanes)
        rolled = pltpu.roll(second[:, columns], lanes // 2, 1)
        tiles.append(jnp.where(low, first[:, columns], rolled))
        tiles.append(jnp.where(low, rolled, first[:, columns]))
    return tiles


def fetch(arrays, buffers, sems):
    copies = []
    for index, (array, buffer) in enumerate(zip(arrays, buffers)):
        copies.append(pltpu.make_async_copy(array, buffer, sems.at[index]))
    for copy in copies:
        copy.start()
    return copies


def turned_into(stage, head, at, tile):
    turned = tile.T.astype(jnp.bfloat16)
    for part in range(tile.shape[0] // lanes):
        begin = at + part * lanes
        stage[head, begin : begin + lanes, :] = turned[:, part * lanes : (part + 1) * lanes]


def key_value_kernel(heads, place, *refs):
    arrays, outs = refs[:6], refs[6 : 6 + heads]
    hidden, query_one, query_two = refs[6 + heads : 9 + heads]
    key_one, key_two, value_proj, stage, sems = refs[9 + heads :]
    buffers = (hidden, key_one, key_two, value_proj, query_one, query_two)
    copies = fetch(arrays, buffers, sems)
    rows = hidden.shape[0]
    copies[0].wait()
    copies[1].wait()
    first = jnp.dot(hidden[...], key_one[...], preferred_element_type=jnp.float32)
    copies[2].wait()
    second = jnp.dot(hidden[...], key_two[...], preferred_element_type=jnp.float32)
    for head, tile in enumerate(pair_up(first, second, heads)):
        stage[head, :rows, :] = tile.astype(jnp.bfloat16)
    copies[3].wait()
    values = jnp.dot(hidden[...], value_proj[...], preferred_element_type=jnp.float32)
    for head in range(heads):
        turned_into(stage, head, rows, values[:, head * lanes : (head + 1) * lanes])
    for turn in range(heads):
        outs[turn][...] = stage[place[0] ^ turn]
    copies[4].wait()
    copies[5].wait()


def query_kernel(heads, scale, place, hidden, query_one, query_two, *refs):
    outs, stage = refs[:heads], refs[heads]
    first = jnp.dot(hidden[...], query_one[...], preferred_element_type=jnp.float32)
    second = jnp.dot(hidden[...], query_two[...], preferred_element_type=jnp.float32)
    for head, tile in enumerate(pair_up(first, second, heads)):
        turned_into(stage, head, 0, tile * scale)
    for turn in range(heads):
        outs[turn][...] = stage[place[0] ^ turn]


def two_maps_of(turned):
    rows = turned.shape[0]
    pieces = [turned[part * lanes : (part + 1) * lanes] for part in range(rows // lanes)]
    joined = jnp.concatenate(pieces, axis=1)
    nothing = jnp.zeros((lanes // 2, rows), jnp.bfloat16)
    low = jnp.concatenate([joined[: lanes // 2], nothing], axis=0)
    high = jnp.concatenate([nothing, joined[lanes // 2 :]], axis=0)
    return jnp.concatenate([low, high], axis=1)


def ahead_of(count, rows):
    key_row = lax.broadcasted_iota(jnp.int32, (count, 2 * rows), 0)
    query_col = lax.broadcasted_iota(jnp.int32, (count, 2 * rows), 1)
    return key_row - jnp.where(query_col < rows, query_col, query_col - rows)


def scores_of(keys, at, count, two_maps):
    return jnp.dot(keys[pl.ds(at, count), :], two_maps, preferred_element_type=jnp.float32)


def weighed(values, at, weights):
    return jnp.dot(
        values[:, pl.ds(at, weights.shape[0])],
        weights.astype(jnp.bfloat16),
        preferred_element_type=jnp.float32,
    )


def fold(weights):
    return jnp.sum(weights.reshape(weights.shape[0] // 8, 8, weights.shape[1]), axis=0)


def span_of(keys, values, at, span, two_maps, limit=None):
    weights = jnp.exp2(scores_of(keys, at, span, two_maps))
    if limit is not None:
        weights = jnp.where(ahead_of(span, two_maps.shape[1] // 2) <= limit, weights, 0.0)
    return weighed(values, at, weights), fold(weights)


def place_block(given, keys, values, at, rows):
    keys[pl.ds(at, rows), :] = given[:rows, :]
    for part in range(rows // lanes):
        begin = rows + part * lanes
        column = pl.multiple_of(at + part * lanes, lanes)
        values[:, pl.ds(column, lanes)] = given[begin : begin + lanes, :]


def early_kernel(heads, down, across, place, *refs):
    z, y, x = place[0], place[1], place[2]
    parts = down * across
    last = heads // 2
    early = [turn for turn in range(heads) if turn != last]
    query_in, refs = refs[:heads], refs[heads:]
    block_in, refs = refs[: len(early) * parts], refs[len(early) * parts :]
    queries, keys, values, accum, sums = refs
    rows = queries.shape[1]
    span = parts * rows

    for turn in range(heads):
        queries[z ^ turn] = query_in[turn][...]
    for below in range(down):
        for aside in range(across):
            for number, turn in enumerate(early):
                block = ((z ^ turn) * down + (y ^ below)) * across + (x ^ aside)
                given = block_in[(below * across + aside) * len(early) + number]
                place_block(given, keys, values, pl.multiple_of(block * rows, rows), rows)

    mine = y * across + x
    for case in range(heads):

        @pl.when(z == case)
        def _(case=case):
            for index in range(heads):
                two_maps = two_maps_of(queries[index])
                added = jnp.zeros(accum.shape[1:], jnp.float32)
                total = jnp.zeros(sums.shape[1:], jnp.float32)
                for at in range(index, -1, -1):
                    if at == case ^ last:
                        continue
                    limit = mine * rows if at == index else None
                    more, weight = span_of(keys, values, at * span, span, two_maps, limit)
                    added = added + more
                    total = total + weight
                accum[index] = added
                sums[index] = total


def late_kernel(heads, down, across, place, lambdas, gain, *refs):
    z, y, x = place[0], place[1], place[2]
    parts = down * across
    last = heads // 2
    block_in, refs = refs[:parts], refs[parts:]
    queries, keys, values, accum, sums = refs[:5]
    outs, refs = refs[5 : 5 + heads], refs[5 + heads :]
    late_keys, late_values, all_keys, all_values, done, flag, added_ref, sums_ref, peak = refs
    rows = queries.shape[1]
    span = parts * rows

    for below in range(down):
        for aside in range(across):
            block = (y ^ below) * across + (x ^ aside)
            given = block_in[below * across + aside]
            at = pl.multiple_of(block * rows, rows)
            place_block(given, late_keys, late_values, at, rows)

    mine = y * across + x
    odd = lax.rem(z, 2) == 1
    lam = lambdas[z]
    weight_low = jnp.where(odd, -lam, 1.0)
    weight_high = jnp.where(odd, 1.0, -lam)

    def finish(index, added, total):
        total = jnp.sum(total, axis=0, keepdims=True)
        heads_out = added * (1.0 / total)
        mixed = heads_out[:, :rows] * weight_low + heads_out[:, rows:] * weight_high
        scale = lax.rsqrt(jnp.mean(mixed * mixed, axis=0, keepdims=True) + epsilon)
        done[index] = ((mixed * scale).T * gain[...]).astype(jnp.bfloat16)
        return total

    flag[...] = jnp.zeros_like(flag)
    for case in range(heads):

        @pl.when(z == case)
        def _(case=case):
            for index in range(heads):
                added, total = accum[index], sums[index]
                if index >= case ^ last:
                    two_maps = two_maps_of(queries[index])
                    limit = mine * rows if index == case ^ last else None
                    more, weight = span_of(late_keys, late_values, 0, span, two_maps, limit)
                    added = added + more
                    total = total + weight
                total = finish(index, added, total)
                inside = (total >= least_sum) & (total <= most_sum)
                flag[...] = jnp.maximum(flag[...], jnp.where(inside, 0.0, 1.0))

    @pl.when(jnp.max(flag[...]) > 0.0)
    def _():
        all_keys[...] = keys[...]
        all_values[...] = values[...]
        begin = pl.multiple_of((z ^ last) * span, span)
        all_keys[pl.ds(begin, span), :] = late_keys[...]
        all_values[:, pl.ds(begin, span)] = late_values[...]

        def redo(index, carried):
            two_maps = two_maps_of(queries[index])
            added_ref[...] = jnp.zeros_like(added_ref)
            sums_ref[...] = jnp.zeros_like(sums_ref)
            peak[...] = jnp.full(peak.shape, masked_score, jnp.float32)

            def one_block(block, inner):
                at = pl.multiple_of(block * rows, rows)
                allowed = ahead_of(rows, rows) <= (index * parts + mine - block) * rows
                scores = jnp.where(allowed, scores_of(all_keys, at, rows, two_maps), masked_score)
                highest = jnp.maximum(peak[...], jnp.max(scores, axis=0, keepdims=True))
                rescale = jnp.exp2(peak[...] - highest)
                weights = jnp.where(allowed, jnp.exp2(scores - highest), 0.0)
                sums_ref[...] = sums_ref[...] * rescale + fold(weights)
                added_ref[...] = added_ref[...] * rescale + weighed(all_values, at, weights)
                peak[...] = highest
                return inner

            lax.fori_loop(0, index * parts + mine + 1, one_block, 0)
            finish(index, added_ref[...], sums_ref[...])
            return carried

        lax.fori_loop(0, heads, redo, 0)

    for turn in range(heads):
        outs[turn][...] = done[z ^ turn]


def project_out_kernel(heads, place, *refs):
    mine, other = refs[:heads], refs[heads : 2 * heads]
    out_mine, out_other, result, joined, staged, sems = refs[2 * heads :]
    z = place[0]
    for turn in range(heads):
        at = pl.multiple_of((z ^ turn) * lanes, lanes)
        joined[0, :, pl.ds(at, lanes)] = mine[turn][...]
        joined[1, :, pl.ds(at, lanes)] = other[turn][...]
    copies = []
    pieces = sems.shape[0]
    wide = result.shape[1] // pieces
    for piece in range(pieces):
        columns = slice(piece * wide, (piece + 1) * wide)
        total = jnp.dot(joined[0], out_mine[:, columns], preferred_element_type=jnp.float32)
        total = total + jnp.dot(
            joined[1], out_other[:, columns], preferred_element_type=jnp.float32
        )
        staged[:, columns] = total.astype(jnp.bfloat16)
        copies.append(
            pltpu.make_async_copy(staged.at[:, columns], result.at[:, columns], sems.at[piece])
        )
        copies[-1].start()
    for copy in copies:
        copy.wait()


def from_hbm(*arrays):
    return [pltpu.with_memory_space_constraint(array, pltpu.HBM) for array in arrays]


def exchanged(
    hidden_in, query_one, query_two, key_one, key_two, value_proj, lambdas, norm_gain, out_proj
):
    heads = lambdas.shape[0]
    groups = lax.axis_size("tp")
    down = across = 2
    parts = down * across
    rows, model = hidden_in.shape
    head_qk = query_one.shape[1] // heads
    width = heads * head_qk
    scale = 1.75 * head_qk ** (-0.5) * log2_e
    bf16 = jnp.bfloat16
    f32 = jnp.float32

    sp_index = lax.axis_index("sp")
    z = sp_index // parts
    y = (sp_index // across) % down
    x = sp_index % across
    place = jnp.stack([z, y, x]).astype(jnp.int32)

    def exchange(array, step):
        pairs = [(index, index ^ step) for index in range(heads * parts)]
        return lax.ppermute(array, "sp", pairs)

    swap_core = [(i, (i + 1) % groups) for i in range(groups)]
    turns = range(heads)

    block_rows = 2 * rows
    block = jax.ShapeDtypeStruct((block_rows, lanes), bf16)
    stripe = jax.ShapeDtypeStruct((rows, lanes), bf16)
    fetched = (hidden_in, query_one, query_two)
    made = pl.pallas_call(
        functools.partial(key_value_kernel, heads),
        out_shape=[block] * heads + [jax.ShapeDtypeStruct(a.shape, bf16) for a in fetched],
        in_specs=[in_smem()] + [in_hbm()] * 6,
        out_specs=[in_vmem()] * (heads + 3),
        scratch_shapes=[
            pltpu.VMEM((model, width), bf16),
            pltpu.VMEM((model, width), bf16),
            pltpu.VMEM((model, heads * lanes), bf16),
            pltpu.VMEM((heads, block_rows, lanes), bf16),
            pltpu.SemaphoreType.DMA((6,)),
        ],
        compiler_params=pltpu.CompilerParams(vmem_limit_bytes=20 << 20),
        cost_estimate=cost(2 * rows * model * 4 * width, 7 << 20),
        name="project_keys",
    )(place, *from_hbm(hidden_in, key_one, key_two, value_proj, query_one, query_two))
    kv, held = made[:heads], made[heads:]
    own = [kv[0]] + [exchange(kv[turn], turn * parts) for turn in turns[1:]]

    queries = pl.pallas_call(
        functools.partial(query_kernel, heads, scale),
        out_shape=[stripe] * heads,
        in_specs=[in_smem()] + [in_vmem()] * 3,
        out_specs=[in_vmem()] * heads,
        scratch_shapes=[pltpu.VMEM((heads, rows, lanes), bf16)],
        compiler_params=pltpu.CompilerParams(vmem_limit_bytes=16 << 20),
        cost_estimate=cost(2 * rows * model * 2 * width, 4 << 20),
        name="project_queries",
    )(place, *held)
    own_queries = [queries[0]]
    for turn in turns[1:]:
        own_queries.append(exchange(queries[turn], turn * parts))

    out_other = lax.ppermute(out_proj, "tp", swap_core)
    aside = [exchange(own[turn], 1) for turn in turns]
    below = [exchange(own[turn], across) for turn in turns]
    corner = [exchange(own[turn], 1 + across) for turn in turns]
    sides = (own, aside, below, corner)
    last = heads // 2
    tokens = heads * rows
    early_blocks = [side[turn] for side in sides for turn in turns if turn != last]
    state = [
        jax.ShapeDtypeStruct((heads, rows, lanes), bf16),
        jax.ShapeDtypeStruct((parts * tokens, lanes), bf16),
        jax.ShapeDtypeStruct((lanes, parts * tokens), bf16),
        jax.ShapeDtypeStruct((heads, lanes, 2 * rows), f32),
        jax.ShapeDtypeStruct((heads, 8, 2 * rows), f32),
    ]
    state = pl.pallas_call(
        functools.partial(early_kernel, heads, down, across),
        out_shape=state,
        in_specs=[in_smem()] + [in_vmem()] * (heads + len(early_blocks)),
        out_specs=[in_vmem()] * 5,
        compiler_params=pltpu.CompilerParams(vmem_limit_bytes=28 << 20),
        cost_estimate=cost(3 * tokens * tokens * parts * lanes, 3 << 20),
        name="attend_early",
    )(place, *own_queries, *early_blocks)
    normed = pl.pallas_call(
        functools.partial(late_kernel, heads, down, across),
        out_shape=[stripe] * heads,
        in_specs=[in_smem()] * 2 + [in_vmem()] * (1 + parts + 5),
        out_specs=[in_vmem()] * heads,
        scratch_shapes=[
            pltpu.VMEM((parts * rows, lanes), bf16),
            pltpu.VMEM((lanes, parts * rows), bf16),
            pltpu.VMEM((parts * tokens, lanes), bf16),
            pltpu.VMEM((lanes, parts * tokens), bf16),
            pltpu.VMEM((heads, rows, lanes), bf16),
            pltpu.VMEM((1, 2 * rows), f32),
            pltpu.VMEM((lanes, 2 * rows), f32),
            pltpu.VMEM((8, 2 * rows), f32),
            pltpu.VMEM((1, 2 * rows), f32),
        ],
        compiler_params=pltpu.CompilerParams(vmem_limit_bytes=28 << 20),
        cost_estimate=cost(tokens * tokens * parts * lanes, 3 << 20),
        name="attend_late",
    )(
        place,
        lambdas,
        norm_gain.reshape(1, lanes),
        *[side[last] for side in sides],
        *state,
    )

    back = [normed[0]]
    for turn in turns[1:]:
        back.append(exchange(normed[turn], turn * parts))
    back_other = [lax.ppermute(back[turn], "tp", swap_core) for turn in turns]
    return pl.pallas_call(
        functools.partial(project_out_kernel, heads),
        out_shape=jax.ShapeDtypeStruct((rows, model), bf16),
        in_specs=[in_smem()] + [in_vmem()] * (2 * heads + 2),
        out_specs=in_hbm(),
        scratch_shapes=[
            pltpu.VMEM((groups, rows, heads * lanes), bf16),
            pltpu.VMEM((rows, model), bf16),
            pltpu.SemaphoreType.DMA((4,)),
        ],
        compiler_params=pltpu.CompilerParams(vmem_limit_bytes=16 << 20),
        cost_estimate=cost(2 * rows * model * groups * heads * lanes, 6 << 20),
        name="project_out",
    )(place, *back, *back_other, out_proj, out_other)


def gathered(
    hidden_in, query_one, query_two, key_one, key_two, value_proj, lambdas, norm_gain, out_proj
):
    heads_dev = lambdas.shape[0]
    head_qk = query_one.shape[1] // heads_dev
    head_v = value_proj.shape[1] // heads_dev
    width_q = heads_dev * head_qk
    score_scale = 1.75 * head_qk ** (-0.5)
    joined = jnp.concatenate((query_one, query_two, key_one, key_two, value_proj), axis=1)
    projected = jnp.dot(hidden_in, joined, preferred_element_type=jnp.float32).astype(jnp.bfloat16)
    tok_rows = projected.shape[0]
    key_values = projected[:, 2 * width_q :]
    my_index = lax.axis_index("sp")
    positions = my_index * tok_rows + jnp.arange(tok_rows, dtype=jnp.int32)
    query_a = projected[:, :width_q].reshape(tok_rows, heads_dev, head_qk)
    query_b = projected[:, width_q : 2 * width_q].reshape(tok_rows, heads_dev, head_qk)
    last_pos = positions[tok_rows - 1]

    def one_map(queries, keys, value_rows, allowed, running_max, running_sum, accum):
        scores = (
            jnp.einsum("qhd,khd->hqk", queries, keys, preferred_element_type=jnp.float32)
            * score_scale
        )
        scores = jnp.where(allowed[None], scores, masked_score)
        new_max = jnp.maximum(running_max, jnp.max(scores, axis=-1))
        rescale = jnp.exp(running_max - new_max)
        weights = jnp.where(allowed[None], jnp.exp(scores - new_max[..., None]), 0.0)
        new_sum = running_sum * rescale + jnp.sum(weights, axis=-1)
        added = jnp.einsum(
            "hqk,khe->hqe",
            weights.astype(jnp.bfloat16),
            value_rows,
            preferred_element_type=jnp.float32,
        )
        return (new_max, new_sum, accum * rescale[..., None] + added)

    def absorb(state, kblock, kstart):
        block_rows = kblock.shape[0]
        k_pos = kstart + jnp.arange(block_rows, dtype=jnp.int32)
        allowed = k_pos[None, :] <= positions[:, None]
        keys_a = kblock[:, :width_q].reshape(block_rows, heads_dev, head_qk)
        keys_b = kblock[:, width_q : 2 * width_q].reshape(block_rows, heads_dev, head_qk)
        value_rows = kblock[:, 2 * width_q :].reshape(block_rows, heads_dev, head_v)
        first_map = one_map(query_a, keys_a, value_rows, allowed, *state[:3])
        second_map = one_map(query_b, keys_b, value_rows, allowed, *state[3:])
        return first_map + second_map

    start_max = jnp.full((heads_dev, tok_rows), masked_score, jnp.float32)
    start_sum = jnp.zeros((heads_dev, tok_rows), jnp.float32)
    start_acc = jnp.zeros((heads_dev, tok_rows, head_v), jnp.float32)
    state = (start_max, start_sum, start_acc, start_max, start_sum, start_acc)
    kv_piece = lax.all_gather(key_values, "sp", axis=0, tiled=True)
    piece_rows = kv_piece.shape[0]
    block_rows = math.gcd(piece_rows, 512)
    block_count = piece_rows // block_rows
    stacked = kv_piece.reshape(block_count, block_rows, kv_piece.shape[1])

    def absorb_step(carried, blocks_in):
        kblock, block_index = blocks_in
        kstart = block_index * block_rows
        renewed = lax.cond(
            kstart <= last_pos,
            lambda inner: absorb(inner, kblock, kstart),
            lambda inner: inner,
            carried,
        )
        return (renewed, None)

    state, _ = lax.scan(absorb_step, state, (stacked, jnp.arange(block_count, dtype=jnp.int32)))
    out_a = state[2] / state[1][..., None]
    out_b = state[5] / state[4][..., None]
    mixed_out = out_a - lambdas[:, None, None] * out_b
    scale_rows = lax.rsqrt(jnp.mean(mixed_out * mixed_out, axis=-1, keepdims=True) + epsilon)
    normed = (mixed_out * scale_rows * norm_gain).astype(jnp.bfloat16)
    normed_all = jnp.transpose(normed, (1, 0, 2)).reshape(tok_rows, heads_dev * head_v)
    partial_value = jnp.dot(normed_all, out_proj, preferred_element_type=jnp.float32)
    return lax.psum(partial_value.astype(jnp.bfloat16), "tp")


def shards(*args):
    hidden_in, query_one, value_proj, lambdas = args[0], args[1], args[5], args[6]
    heads = lambdas.shape[0]
    groups, length = lax.axis_size("tp"), lax.axis_size("sp")
    fits = (
        groups == 2
        and heads == 4
        and length == 4 * heads
        and query_one.shape[1] == heads * (lanes // 2)
        and value_proj.shape[1] == heads * lanes
        and hidden_in.shape[0] % lanes == 0
        and hidden_in.shape[0] <= 512
    )
    if not fits:
        return gathered(*args)
    return exchanged(*args)


def solution(mesh):
    placed = (
        P("sp", None),
        P(None, "tp"),
        P(None, "tp"),
        P(None, "tp"),
        P(None, "tp"),
        P(None, "tp"),
        P("tp"),
        P(),
        P("tp", None),
    )
    return jax.shard_map(
        shards, mesh=mesh, in_specs=placed, out_specs=P("sp", None), check_vma=False
    )
```

```python
import functools
import math

import jax
import jax.numpy as jnp
from jax import lax
from jax.experimental import pallas as pl
from jax.experimental.pallas import tpu as pltpu
from jax.sharding import PartitionSpec as P


epsilon = 1e-06
masked_score = -1e30
log2_e = 1.4426950408889634
least_sum = 2.0**-90
most_sum = 2.0**100
lanes = 128
key_pieces = 4
start_queries = 0


def cost(flops, moved):
    return pl.CostEstimate(flops=int(flops), bytes_accessed=int(moved), transcendentals=0)


def in_vmem():
    return pl.BlockSpec(memory_space=pltpu.VMEM)


def in_smem():
    return pl.BlockSpec(memory_space=pltpu.SMEM)


def in_hbm():
    return pl.BlockSpec(memory_space=pltpu.HBM)


def pair_up(first, second, heads):
    tiles = []
    low = lax.broadcasted_iota(jnp.int32, (first.shape[0], lanes), 1) < lanes // 2
    for pair in range(heads // 2):
        columns = slice(pair * lanes, (pair + 1) * lanes)
        rolled = pltpu.roll(second[:, columns], lanes // 2, 1)
        tiles.append(jnp.where(low, first[:, columns], rolled))
        tiles.append(jnp.where(low, rolled, first[:, columns]))
    return tiles


def fetch_later(arrays, buffers, sems, row):
    return [
        pltpu.make_async_copy(array, buffer, sems.at[row, number])
        for number, (array, buffer) in enumerate(zip(arrays, buffers))
    ]


def turned_into(stage, head, at, tile):
    turned = tile.T.astype(jnp.bfloat16)
    for part in range(tile.shape[0] // lanes):
        begin = at + part * lanes
        stage[head, begin : begin + lanes, :] = turned[:, part * lanes : (part + 1) * lanes]


def key_value_kernel(heads, place, *refs):
    arrays, outs = refs[:6], refs[6 : 6 + heads]
    hidden, query_one, query_two = refs[6 + heads : 9 + heads]
    key_one, key_two, value_proj, stage, sems = refs[9 + heads :]
    rows, model = hidden.shape
    pieces = sems.shape[0] - 1
    deep = model // pieces
    copies = []
    for piece in range(pieces):
        cut = slice(piece * deep, (piece + 1) * deep)
        pairs = [(arrays[0].at[:, cut], hidden.at[:, cut])]
        for array, buffer in zip(arrays[1:4], (key_one, key_two, value_proj)):
            pairs.append((array.at[cut, :], buffer.at[cut, :]))
        for number, (source, target) in enumerate(pairs):
            copies.append(pltpu.make_async_copy(source, target, sems.at[piece, number]))
            copies[-1].start()
    later = fetch_later(arrays[4:], (query_one, query_two), sems, pieces)
    sums = [0.0, 0.0, 0.0]
    for piece in range(pieces):
        for copy in copies[4 * piece : 4 * piece + 4]:
            copy.wait()
        if piece == start_queries:
            for copy in later:
                copy.start()
        cut = slice(piece * deep, (piece + 1) * deep)
        tokens = hidden[:, cut]
        for number, buffer in enumerate((key_one, key_two, value_proj)):
            sums[number] += jnp.dot(tokens, buffer[cut, :], preferred_element_type=jnp.float32)
    first, second, values = sums
    for head, tile in enumerate(pair_up(first, second, heads)):
        stage[head, :rows, :] = tile.astype(jnp.bfloat16)
    for head in range(heads):
        turned_into(stage, head, rows, values[:, head * lanes : (head + 1) * lanes])
    for turn in range(heads):
        outs[turn][...] = stage[place[0] ^ turn]
    for copy in later:
        copy.wait()


def query_kernel(heads, place, hidden, query_one, query_two, *refs):
    outs, stage = refs[:heads], refs[heads]
    first = jnp.dot(hidden[...], query_one[...], preferred_element_type=jnp.float32)
    second = jnp.dot(hidden[...], query_two[...], preferred_element_type=jnp.float32)
    for head, tile in enumerate(pair_up(first, second, heads)):
        turned_into(stage, head, 0, tile)
    for turn in range(heads):
        outs[turn][...] = stage[place[0] ^ turn]


def two_maps_of(turned):
    rows = turned.shape[0]
    pieces = [turned[part * lanes : (part + 1) * lanes] for part in range(rows // lanes)]
    joined = jnp.concatenate(pieces, axis=1)
    nothing = jnp.zeros((lanes // 2, rows), jnp.bfloat16)
    low = jnp.concatenate([joined[: lanes // 2], nothing], axis=0)
    high = jnp.concatenate([nothing, joined[lanes // 2 :]], axis=0)
    return jnp.concatenate([low, high], axis=1)


def ahead_of(count, rows):
    key_row = lax.broadcasted_iota(jnp.int32, (count, 2 * rows), 0)
    query_col = lax.broadcasted_iota(jnp.int32, (count, 2 * rows), 1)
    return key_row - jnp.where(query_col < rows, query_col, query_col - rows)


def scores_of(keys, at, count, two_maps):
    return jnp.dot(keys[pl.ds(at, count), :], two_maps, preferred_element_type=jnp.float32)


def weighed(values, at, weights):
    return jnp.dot(
        values[:, pl.ds(at, weights.shape[0])],
        weights.astype(jnp.bfloat16),
        preferred_element_type=jnp.float32,
    )


def fold(weights):
    return jnp.sum(weights.reshape(weights.shape[0] // 8, 8, weights.shape[1]), axis=0)


def span_of(scale, keys, values, at, span, two_maps, limit=None):
    weights = jnp.exp2(scores_of(keys, at, span, two_maps) * scale)
    if limit is not None:
        weights = jnp.where(ahead_of(span, two_maps.shape[1] // 2) <= limit, weights, 0.0)
    return weighed(values, at, weights), fold(weights)


def place_block(given, keys, values, at, rows):
    keys[pl.ds(at, rows), :] = given[:rows, :]
    for part in range(rows // lanes):
        begin = rows + part * lanes
        column = pl.multiple_of(at + part * lanes, lanes)
        values[:, pl.ds(column, lanes)] = given[begin : begin + lanes, :]


def early_kernel(scale, heads, down, across, place, *refs):
    z, y, x = place[0], place[1], place[2]
    parts = down * across
    last = heads // 2
    early = [turn for turn in range(heads) if turn != last]
    query_in, refs = refs[:heads], refs[heads:]
    block_in, refs = refs[: len(early) * parts], refs[len(early) * parts :]
    queries, keys, values, accum, sums = refs
    rows = queries.shape[1]
    span = parts * rows

    for turn in range(heads):
        queries[z ^ turn] = query_in[turn][...]
    for below in range(down):
        for aside in range(across):
            for number, turn in enumerate(early):
                block = ((z ^ turn) * down + (y ^ below)) * across + (x ^ aside)
                given = block_in[(below * across + aside) * len(early) + number]
                place_block(given, keys, values, pl.multiple_of(block * rows, rows), rows)

    mine = y * across + x
    for case in range(heads):

        @pl.when(z == case)
        def _(case=case):
            for index in range(heads):
                two_maps = two_maps_of(queries[index])
                added = jnp.zeros(accum.shape[1:], jnp.float32)
                total = jnp.zeros(sums.shape[1:], jnp.float32)
                for at in range(index, -1, -1):
                    if at == case ^ last:
                        continue
                    limit = mine * rows if at == index else None
                    more, weight = span_of(scale, keys, values, at * span, span, two_maps, limit)
                    added = added + more
                    total = total + weight
                accum[index] = added
                sums[index] = total


def late_kernel(scale, heads, down, across, place, lambdas, gain, *refs):
    z, y, x = place[0], place[1], place[2]
    parts = down * across
    last = heads // 2
    block_in, refs = refs[:parts], refs[parts:]
    queries, keys, values, accum, sums = refs[:5]
    outs, refs = refs[5 : 5 + heads], refs[5 + heads :]
    late_keys, late_values, all_keys, all_values, done, flag, added_ref, sums_ref, peak = refs
    rows = queries.shape[1]
    span = parts * rows

    for below in range(down):
        for aside in range(across):
            block = (y ^ below) * across + (x ^ aside)
            given = block_in[below * across + aside]
            at = pl.multiple_of(block * rows, rows)
            place_block(given, late_keys, late_values, at, rows)

    mine = y * across + x
    odd = lax.rem(z, 2) == 1
    lam = lambdas[z]
    weight_low = jnp.where(odd, -lam, 1.0)
    weight_high = jnp.where(odd, 1.0, -lam)

    def finish(index, added, total):
        total = jnp.sum(total, axis=0, keepdims=True)
        heads_out = added * (1.0 / total)
        mixed = heads_out[:, :rows] * weight_low + heads_out[:, rows:] * weight_high
        scale = lax.rsqrt(jnp.mean(mixed * mixed, axis=0, keepdims=True) + epsilon)
        done[index] = ((mixed * scale).T * gain[...]).astype(jnp.bfloat16)
        return total

    flag[...] = jnp.zeros_like(flag)
    for case in range(heads):

        @pl.when(z == case)
        def _(case=case):
            for index in range(heads):
                added, total = accum[index], sums[index]
                if index >= case ^ last:
                    two_maps = two_maps_of(queries[index])
                    limit = mine * rows if index == case ^ last else None
                    more, weight = span_of(
                        scale, late_keys, late_values, 0, span, two_maps, limit
                    )
                    added = added + more
                    total = total + weight
                total = finish(index, added, total)
                inside = (total >= least_sum) & (total <= most_sum)
                flag[...] = jnp.maximum(flag[...], jnp.where(inside, 0.0, 1.0))

    @pl.when(jnp.max(flag[...]) > 0.0)
    def _():
        all_keys[...] = keys[...]
        all_values[...] = values[...]
        begin = pl.multiple_of((z ^ last) * span, span)
        all_keys[pl.ds(begin, span), :] = late_keys[...]
        all_values[:, pl.ds(begin, span)] = late_values[...]

        def redo(index, carried):
            two_maps = two_maps_of(queries[index])
            added_ref[...] = jnp.zeros_like(added_ref)
            sums_ref[...] = jnp.zeros_like(sums_ref)
            peak[...] = jnp.full(peak.shape, masked_score, jnp.float32)

            def one_block(block, inner):
                at = pl.multiple_of(block * rows, rows)
                allowed = ahead_of(rows, rows) <= (index * parts + mine - block) * rows
                scores = scores_of(all_keys, at, rows, two_maps) * scale
                scores = jnp.where(allowed, scores, masked_score)
                highest = jnp.maximum(peak[...], jnp.max(scores, axis=0, keepdims=True))
                rescale = jnp.exp2(peak[...] - highest)
                weights = jnp.where(allowed, jnp.exp2(scores - highest), 0.0)
                sums_ref[...] = sums_ref[...] * rescale + fold(weights)
                added_ref[...] = added_ref[...] * rescale + weighed(all_values, at, weights)
                peak[...] = highest
                return inner

            lax.fori_loop(0, index * parts + mine + 1, one_block, 0)
            finish(index, added_ref[...], sums_ref[...])
            return carried

        lax.fori_loop(0, heads, redo, 0)

    for turn in range(heads):
        outs[turn][...] = done[z ^ turn]


def project_out_kernel(heads, place, *refs):
    mine, other = refs[:heads], refs[heads : 2 * heads]
    out_mine, out_other, result, joined, staged, sems = refs[2 * heads :]
    z = place[0]
    for turn in range(heads):
        at = pl.multiple_of((z ^ turn) * lanes, lanes)
        joined[0, :, pl.ds(at, lanes)] = mine[turn][...]
        joined[1, :, pl.ds(at, lanes)] = other[turn][...]
    copies = []
    pieces = sems.shape[0]
    wide = result.shape[1] // pieces
    for piece in range(pieces):
        columns = slice(piece * wide, (piece + 1) * wide)
        total = jnp.dot(joined[0], out_mine[:, columns], preferred_element_type=jnp.float32)
        total = total + jnp.dot(
            joined[1], out_other[:, columns], preferred_element_type=jnp.float32
        )
        staged[:, columns] = total.astype(jnp.bfloat16)
        copies.append(
            pltpu.make_async_copy(staged.at[:, columns], result.at[:, columns], sems.at[piece])
        )
        copies[-1].start()
    for copy in copies:
        copy.wait()


def from_hbm(*arrays):
    return [pltpu.with_memory_space_constraint(array, pltpu.HBM) for array in arrays]


def exchanged(
    hidden_in, query_one, query_two, key_one, key_two, value_proj, lambdas, norm_gain, out_proj
):
    heads = lambdas.shape[0]
    groups = lax.axis_size("tp")
    down = across = 2
    parts = down * across
    rows, model = hidden_in.shape
    head_qk = query_one.shape[1] // heads
    width = heads * head_qk
    scale = 1.75 * head_qk ** (-0.5) * log2_e
    bf16 = jnp.bfloat16
    f32 = jnp.float32

    sp_index = lax.axis_index("sp")
    z = sp_index // parts
    y = (sp_index // across) % down
    x = sp_index % across
    place = jnp.stack([z, y, x]).astype(jnp.int32)

    def exchange(array, step):
        pairs = [(index, index ^ step) for index in range(heads * parts)]
        return lax.ppermute(array, "sp", pairs)

    swap_core = [(i, (i + 1) % groups) for i in range(groups)]
    turns = range(heads)

    block_rows = 2 * rows
    block = jax.ShapeDtypeStruct((block_rows, lanes), bf16)
    stripe = jax.ShapeDtypeStruct((rows, lanes), bf16)
    fetched = (hidden_in, query_one, query_two)
    made = pl.pallas_call(
        functools.partial(key_value_kernel, heads),
        out_shape=[block] * heads + [jax.ShapeDtypeStruct(a.shape, bf16) for a in fetched],
        in_specs=[in_smem()] + [in_hbm()] * 6,
        out_specs=[in_vmem()] * (heads + 3),
        scratch_shapes=[
            pltpu.VMEM((model, width), bf16),
            pltpu.VMEM((model, width), bf16),
            pltpu.VMEM((model, heads * lanes), bf16),
            pltpu.VMEM((heads, block_rows, lanes), bf16),
            pltpu.SemaphoreType.DMA((key_pieces + 1, 4)),
        ],
        compiler_params=pltpu.CompilerParams(vmem_limit_bytes=20 << 20),
        cost_estimate=cost(2 * rows * model * 4 * width, 7 << 20),
        name="project_keys",
    )(place, *from_hbm(hidden_in, key_one, key_two, value_proj, query_one, query_two))
    kv, held = made[:heads], made[heads:]
    own = [kv[0]] + [exchange(kv[turn], turn * parts) for turn in turns[1:]]

    queries = pl.pallas_call(
        functools.partial(query_kernel, heads),
        out_shape=[stripe] * heads,
        in_specs=[in_smem()] + [in_vmem()] * 3,
        out_specs=[in_vmem()] * heads,
        scratch_shapes=[pltpu.VMEM((heads, rows, lanes), bf16)],
        compiler_params=pltpu.CompilerParams(vmem_limit_bytes=16 << 20),
        cost_estimate=cost(2 * rows * model * 2 * width, 4 << 20),
        name="project_queries",
    )(place, *held)
    own_queries = [queries[0]]
    for turn in turns[1:]:
        own_queries.append(exchange(queries[turn], turn * parts))

    out_other = lax.ppermute(out_proj, "tp", swap_core)
    aside = [exchange(own[turn], 1) for turn in turns]
    below = [exchange(own[turn], across) for turn in turns]
    corner = [exchange(own[turn], 1 + across) for turn in turns]
    sides = (own, aside, below, corner)
    last = heads // 2
    tokens = heads * rows
    early_blocks = [side[turn] for side in sides for turn in turns if turn != last]
    state = [
        jax.ShapeDtypeStruct((heads, rows, lanes), bf16),
        jax.ShapeDtypeStruct((parts * tokens, lanes), bf16),
        jax.ShapeDtypeStruct((lanes, parts * tokens), bf16),
        jax.ShapeDtypeStruct((heads, lanes, 2 * rows), f32),
        jax.ShapeDtypeStruct((heads, 8, 2 * rows), f32),
    ]
    state = pl.pallas_call(
        functools.partial(early_kernel, scale, heads, down, across),
        out_shape=state,
        in_specs=[in_smem()] + [in_vmem()] * (heads + len(early_blocks)),
        out_specs=[in_vmem()] * 5,
        compiler_params=pltpu.CompilerParams(vmem_limit_bytes=28 << 20),
        cost_estimate=cost(3 * tokens * tokens * parts * lanes, 3 << 20),
        name="attend_early",
    )(place, *own_queries, *early_blocks)
    normed = pl.pallas_call(
        functools.partial(late_kernel, scale, heads, down, across),
        out_shape=[stripe] * heads,
        in_specs=[in_smem()] * 2 + [in_vmem()] * (1 + parts + 5),
        out_specs=[in_vmem()] * heads,
        scratch_shapes=[
            pltpu.VMEM((parts * rows, lanes), bf16),
            pltpu.VMEM((lanes, parts * rows), bf16),
            pltpu.VMEM((parts * tokens, lanes), bf16),
            pltpu.VMEM((lanes, parts * tokens), bf16),
            pltpu.VMEM((heads, rows, lanes), bf16),
            pltpu.VMEM((1, 2 * rows), f32),
            pltpu.VMEM((lanes, 2 * rows), f32),
            pltpu.VMEM((8, 2 * rows), f32),
            pltpu.VMEM((1, 2 * rows), f32),
        ],
        compiler_params=pltpu.CompilerParams(vmem_limit_bytes=28 << 20),
        cost_estimate=cost(tokens * tokens * parts * lanes, 3 << 20),
        name="attend_late",
    )(
        place,
        lambdas,
        norm_gain.reshape(1, lanes),
        *[side[last] for side in sides],
        *state,
    )

    back = [normed[0]]
    for turn in turns[1:]:
        back.append(exchange(normed[turn], turn * parts))
    back_other = [lax.ppermute(back[turn], "tp", swap_core) for turn in turns]
    return pl.pallas_call(
        functools.partial(project_out_kernel, heads),
        out_shape=jax.ShapeDtypeStruct((rows, model), bf16),
        in_specs=[in_smem()] + [in_vmem()] * (2 * heads + 2),
        out_specs=in_hbm(),
        scratch_shapes=[
            pltpu.VMEM((groups, rows, heads * lanes), bf16),
            pltpu.VMEM((rows, model), bf16),
            pltpu.SemaphoreType.DMA((4,)),
        ],
        compiler_params=pltpu.CompilerParams(vmem_limit_bytes=16 << 20),
        cost_estimate=cost(2 * rows * model * groups * heads * lanes, 6 << 20),
        name="project_out",
    )(place, *back, *back_other, out_proj, out_other)


def gathered(
    hidden_in, query_one, query_two, key_one, key_two, value_proj, lambdas, norm_gain, out_proj
):
    heads_dev = lambdas.shape[0]
    head_qk = query_one.shape[1] // heads_dev
    head_v = value_proj.shape[1] // heads_dev
    width_q = heads_dev * head_qk
    score_scale = 1.75 * head_qk ** (-0.5)
    joined = jnp.concatenate((query_one, query_two, key_one, key_two, value_proj), axis=1)
    projected = jnp.dot(hidden_in, joined, preferred_element_type=jnp.float32).astype(jnp.bfloat16)
    tok_rows = projected.shape[0]
    key_values = projected[:, 2 * width_q :]
    my_index = lax.axis_index("sp")
    positions = my_index * tok_rows + jnp.arange(tok_rows, dtype=jnp.int32)
    query_a = projected[:, :width_q].reshape(tok_rows, heads_dev, head_qk)
    query_b = projected[:, width_q : 2 * width_q].reshape(tok_rows, heads_dev, head_qk)
    last_pos = positions[tok_rows - 1]

    def one_map(queries, keys, value_rows, allowed, running_max, running_sum, accum):
        scores = (
            jnp.einsum("qhd,khd->hqk", queries, keys, preferred_element_type=jnp.float32)
            * score_scale
        )
        scores = jnp.where(allowed[None], scores, masked_score)
        new_max = jnp.maximum(running_max, jnp.max(scores, axis=-1))
        rescale = jnp.exp(running_max - new_max)
        weights = jnp.where(allowed[None], jnp.exp(scores - new_max[..., None]), 0.0)
        new_sum = running_sum * rescale + jnp.sum(weights, axis=-1)
        added = jnp.einsum(
            "hqk,khe->hqe",
            weights.astype(jnp.bfloat16),
            value_rows,
            preferred_element_type=jnp.float32,
        )
        return (new_max, new_sum, accum * rescale[..., None] + added)

    def absorb(state, kblock, kstart):
        block_rows = kblock.shape[0]
        k_pos = kstart + jnp.arange(block_rows, dtype=jnp.int32)
        allowed = k_pos[None, :] <= positions[:, None]
        keys_a = kblock[:, :width_q].reshape(block_rows, heads_dev, head_qk)
        keys_b = kblock[:, width_q : 2 * width_q].reshape(block_rows, heads_dev, head_qk)
        value_rows = kblock[:, 2 * width_q :].reshape(block_rows, heads_dev, head_v)
        first_map = one_map(query_a, keys_a, value_rows, allowed, *state[:3])
        second_map = one_map(query_b, keys_b, value_rows, allowed, *state[3:])
        return first_map + second_map

    start_max = jnp.full((heads_dev, tok_rows), masked_score, jnp.float32)
    start_sum = jnp.zeros((heads_dev, tok_rows), jnp.float32)
    start_acc = jnp.zeros((heads_dev, tok_rows, head_v), jnp.float32)
    state = (start_max, start_sum, start_acc, start_max, start_sum, start_acc)
    kv_piece = lax.all_gather(key_values, "sp", axis=0, tiled=True)
    piece_rows = kv_piece.shape[0]
    block_rows = math.gcd(piece_rows, 512)
    block_count = piece_rows // block_rows
    stacked = kv_piece.reshape(block_count, block_rows, kv_piece.shape[1])

    def absorb_step(carried, blocks_in):
        kblock, block_index = blocks_in
        kstart = block_index * block_rows
        renewed = lax.cond(
            kstart <= last_pos,
            lambda inner: absorb(inner, kblock, kstart),
            lambda inner: inner,
            carried,
        )
        return (renewed, None)

    state, _ = lax.scan(absorb_step, state, (stacked, jnp.arange(block_count, dtype=jnp.int32)))
    out_a = state[2] / state[1][..., None]
    out_b = state[5] / state[4][..., None]
    mixed_out = out_a - lambdas[:, None, None] * out_b
    scale_rows = lax.rsqrt(jnp.mean(mixed_out * mixed_out, axis=-1, keepdims=True) + epsilon)
    normed = (mixed_out * scale_rows * norm_gain).astype(jnp.bfloat16)
    normed_all = jnp.transpose(normed, (1, 0, 2)).reshape(tok_rows, heads_dev * head_v)
    partial_value = jnp.dot(normed_all, out_proj, preferred_element_type=jnp.float32)
    return lax.psum(partial_value.astype(jnp.bfloat16), "tp")


def shards(*args):
    hidden_in, query_one, value_proj, lambdas = args[0], args[1], args[5], args[6]
    heads = lambdas.shape[0]
    groups, length = lax.axis_size("tp"), lax.axis_size("sp")
    fits = (
        groups == 2
        and heads == 4
        and length == 4 * heads
        and query_one.shape[1] == heads * (lanes // 2)
        and value_proj.shape[1] == heads * lanes
        and hidden_in.shape[0] % lanes == 0
        and hidden_in.shape[0] <= 512
    )
    if not fits:
        return gathered(*args)
    return exchanged(*args)


def solution(mesh):
    placed = (
        P("sp", None),
        P(None, "tp"),
        P(None, "tp"),
        P(None, "tp"),
        P(None, "tp"),
        P(None, "tp"),
        P("tp"),
        P(),
        P("tp", None),
    )
    return jax.shard_map(
        shards, mesh=mesh, in_specs=placed, out_specs=P("sp", None), check_vma=False
    )
```

```python
import functools
import math

import jax
import jax.numpy as jnp
from jax import lax
from jax.experimental import pallas as pl
from jax.experimental.pallas import tpu as pltpu
from jax.sharding import PartitionSpec as P


epsilon = 1e-06
masked_score = -1e30
log2_e = 1.4426950408889634
least_sum = 2.0**-90
most_sum = 2.0**100
lanes = 128
key_pieces = 4
riding = None
apart = (0, 1, 2, 3)


def cost(flops, moved):
    return pl.CostEstimate(flops=int(flops), bytes_accessed=int(moved), transcendentals=0)


def in_vmem():
    return pl.BlockSpec(memory_space=pltpu.VMEM)


def in_smem():
    return pl.BlockSpec(memory_space=pltpu.SMEM)


def in_hbm():
    return pl.BlockSpec(memory_space=pltpu.HBM)


def pair_up(first, second, heads):
    tiles = []
    low = lax.broadcasted_iota(jnp.int32, (first.shape[0], lanes), 1) < lanes // 2
    for pair in range(heads // 2):
        columns = slice(pair * lanes, (pair + 1) * lanes)
        rolled = pltpu.roll(second[:, columns], lanes // 2, 1)
        tiles.append(jnp.where(low, first[:, columns], rolled))
        tiles.append(jnp.where(low, rolled, first[:, columns]))
    return tiles


def turned_into(stage, head, at, tile):
    turned = tile.T.astype(jnp.bfloat16)
    for part in range(tile.shape[0] // lanes):
        begin = at + part * lanes
        stage[head, begin : begin + lanes, :] = turned[:, part * lanes : (part + 1) * lanes]


def project_kernel(heads, place, *refs):
    arrays, outs = refs[:6], refs[6 : 6 + heads]
    query_outs, refs = refs[6 + heads : 6 + heads + len(apart)], refs[6 + heads + len(apart) :]
    buffers, stage, query_stage, sems = refs[:6], refs[6], refs[7], refs[8]
    rows, model = buffers[0].shape
    pieces = sems.shape[0]
    deep = model // pieces
    copies = []
    for piece in range(pieces):
        cut = slice(piece * deep, (piece + 1) * deep)
        for number, (array, buffer) in enumerate(zip(arrays, buffers)):
            source = array.at[cut, :] if number else array.at[:, cut]
            target = buffer.at[cut, :] if number else buffer.at[:, cut]
            copies.append(pltpu.make_async_copy(source, target, sems.at[piece, number]))
            copies[-1].start()
    sums = [0.0] * 5
    for piece in range(pieces):
        for copy in copies[6 * piece : 6 * piece + 6]:
            copy.wait()
        cut = slice(piece * deep, (piece + 1) * deep)
        tokens = buffers[0][:, cut]
        for number, buffer in enumerate(buffers[1:]):
            sums[number] += jnp.dot(tokens, buffer[cut, :], preferred_element_type=jnp.float32)
    for head, tile in enumerate(pair_up(sums[0], sums[1], heads)):
        stage[head, :rows, :] = tile.astype(jnp.bfloat16)
    for head in range(heads):
        turned_into(stage, head, rows, sums[2][:, head * lanes : (head + 1) * lanes])
    for head, tile in enumerate(pair_up(sums[3], sums[4], heads)):
        turned_into(query_stage, head, 0, tile)
    taken = stage.shape[1]
    for turn in range(heads):
        if turn == riding:
            outs[turn][:taken, :] = stage[place[0] ^ turn]
            outs[turn][taken:, :] = query_stage[place[0] ^ turn]
        else:
            outs[turn][...] = stage[place[0] ^ turn]
            query_outs[apart.index(turn)][...] = query_stage[place[0] ^ turn]


def two_maps_of(turned):
    rows = turned.shape[0]
    pieces = [turned[part * lanes : (part + 1) * lanes] for part in range(rows // lanes)]
    joined = jnp.concatenate(pieces, axis=1)
    nothing = jnp.zeros((lanes // 2, rows), jnp.bfloat16)
    low = jnp.concatenate([joined[: lanes // 2], nothing], axis=0)
    high = jnp.concatenate([nothing, joined[lanes // 2 :]], axis=0)
    return jnp.concatenate([low, high], axis=1)


def ahead_of(count, rows):
    key_row = lax.broadcasted_iota(jnp.int32, (count, 2 * rows), 0)
    query_col = lax.broadcasted_iota(jnp.int32, (count, 2 * rows), 1)
    return key_row - jnp.where(query_col < rows, query_col, query_col - rows)


def scores_of(keys, at, count, two_maps):
    return jnp.dot(keys[pl.ds(at, count), :], two_maps, preferred_element_type=jnp.float32)


def weighed(values, at, weights):
    return jnp.dot(
        values[:, pl.ds(at, weights.shape[0])],
        weights.astype(jnp.bfloat16),
        preferred_element_type=jnp.float32,
    )


def fold(weights):
    return jnp.sum(weights.reshape(weights.shape[0] // 8, 8, weights.shape[1]), axis=0)


def span_of(scale, keys, values, at, span, two_maps, limit=None):
    weights = jnp.exp2(scores_of(keys, at, span, two_maps) * scale)
    if limit is not None:
        weights = jnp.where(ahead_of(span, two_maps.shape[1] // 2) <= limit, weights, 0.0)
    return weighed(values, at, weights), fold(weights)


def place_block(given, keys, values, at, rows):
    keys[pl.ds(at, rows), :] = given[:rows, :]
    for part in range(rows // lanes):
        begin = rows + part * lanes
        column = pl.multiple_of(at + part * lanes, lanes)
        values[:, pl.ds(column, lanes)] = given[begin : begin + lanes, :]


def early_kernel(scale, heads, down, across, place, *refs):
    z, y, x = place[0], place[1], place[2]
    parts = down * across
    last = heads // 2
    early = [turn for turn in range(heads) if turn != last]
    query_in, refs = refs[: len(apart)], refs[len(apart) :]
    block_in, refs = refs[: len(early) * parts], refs[len(early) * parts :]
    queries, keys, values, accum, sums = refs
    rows = queries.shape[1]
    span = parts * rows

    for turn in range(heads):
        if turn == riding:
            queries[z ^ turn] = block_in[early.index(turn)][2 * rows :, :]
        else:
            queries[z ^ turn] = query_in[apart.index(turn)][...]
    for below in range(down):
        for aside in range(across):
            for number, turn in enumerate(early):
                block = ((z ^ turn) * down + (y ^ below)) * across + (x ^ aside)
                given = block_in[(below * across + aside) * len(early) + number]
                place_block(given, keys, values, pl.multiple_of(block * rows, rows), rows)

    mine = y * across + x
    for case in range(heads):

        @pl.when(z == case)
        def _(case=case):
            for index in range(heads):
                two_maps = two_maps_of(queries[index])
                added = jnp.zeros(accum.shape[1:], jnp.float32)
                total = jnp.zeros(sums.shape[1:], jnp.float32)
                for at in range(index, -1, -1):
                    if at == case ^ last:
                        continue
                    limit = mine * rows if at == index else None
                    more, weight = span_of(scale, keys, values, at * span, span, two_maps, limit)
                    added = added + more
                    total = total + weight
                accum[index] = added
                sums[index] = total


def late_kernel(scale, heads, down, across, place, lambdas, gain, *refs):
    z, y, x = place[0], place[1], place[2]
    parts = down * across
    last = heads // 2
    block_in, refs = refs[:parts], refs[parts:]
    queries, keys, values, accum, sums = refs[:5]
    outs, refs = refs[5 : 5 + heads], refs[5 + heads :]
    late_keys, late_values, all_keys, all_values, done, flag, added_ref, sums_ref, peak = refs
    rows = queries.shape[1]
    span = parts * rows

    for below in range(down):
        for aside in range(across):
            block = (y ^ below) * across + (x ^ aside)
            given = block_in[below * across + aside]
            at = pl.multiple_of(block * rows, rows)
            place_block(given, late_keys, late_values, at, rows)

    mine = y * across + x
    odd = lax.rem(z, 2) == 1
    lam = lambdas[z]
    weight_low = jnp.where(odd, -lam, 1.0)
    weight_high = jnp.where(odd, 1.0, -lam)

    def finish(index, added, total):
        total = jnp.sum(total, axis=0, keepdims=True)
        heads_out = added * (1.0 / total)
        mixed = heads_out[:, :rows] * weight_low + heads_out[:, rows:] * weight_high
        scale = lax.rsqrt(jnp.mean(mixed * mixed, axis=0, keepdims=True) + epsilon)
        done[index] = ((mixed * scale).T * gain[...]).astype(jnp.bfloat16)
        return total

    flag[...] = jnp.zeros_like(flag)
    for case in range(heads):

        @pl.when(z == case)
        def _(case=case):
            for index in range(heads):
                added, total = accum[index], sums[index]
                if index >= case ^ last:
                    two_maps = two_maps_of(queries[index])
                    limit = mine * rows if index == case ^ last else None
                    more, weight = span_of(
                        scale, late_keys, late_values, 0, span, two_maps, limit
                    )
                    added = added + more
                    total = total + weight
                total = finish(index, added, total)
                inside = (total >= least_sum) & (total <= most_sum)
                flag[...] = jnp.maximum(flag[...], jnp.where(inside, 0.0, 1.0))

    @pl.when(jnp.max(flag[...]) > 0.0)
    def _():
        all_keys[...] = keys[...]
        all_values[...] = values[...]
        begin = pl.multiple_of((z ^ last) * span, span)
        all_keys[pl.ds(begin, span), :] = late_keys[...]
        all_values[:, pl.ds(begin, span)] = late_values[...]

        def redo(index, carried):
            two_maps = two_maps_of(queries[index])
            added_ref[...] = jnp.zeros_like(added_ref)
            sums_ref[...] = jnp.zeros_like(sums_ref)
            peak[...] = jnp.full(peak.shape, masked_score, jnp.float32)

            def one_block(block, inner):
                at = pl.multiple_of(block * rows, rows)
                allowed = ahead_of(rows, rows) <= (index * parts + mine - block) * rows
                scores = scores_of(all_keys, at, rows, two_maps) * scale
                scores = jnp.where(allowed, scores, masked_score)
                highest = jnp.maximum(peak[...], jnp.max(scores, axis=0, keepdims=True))
                rescale = jnp.exp2(peak[...] - highest)
                weights = jnp.where(allowed, jnp.exp2(scores - highest), 0.0)
                sums_ref[...] = sums_ref[...] * rescale + fold(weights)
                added_ref[...] = added_ref[...] * rescale + weighed(all_values, at, weights)
                peak[...] = highest
                return inner

            lax.fori_loop(0, index * parts + mine + 1, one_block, 0)
            finish(index, added_ref[...], sums_ref[...])
            return carried

        lax.fori_loop(0, heads, redo, 0)

    for turn in range(heads):
        outs[turn][...] = done[z ^ turn]


def project_out_kernel(heads, place, *refs):
    mine, other = refs[:heads], refs[heads : 2 * heads]
    out_mine, out_other, result, joined, staged, sems = refs[2 * heads :]
    z = place[0]
    for turn in range(heads):
        joined[0, z ^ turn] = mine[turn][...]
        joined[1, z ^ turn] = other[turn][...]
    first = jnp.concatenate([joined[0, head] for head in range(heads)], axis=1)
    second = jnp.concatenate([joined[1, head] for head in range(heads)], axis=1)
    copies = []
    pieces = sems.shape[0]
    wide = result.shape[1] // pieces
    for piece in range(pieces):
        columns = slice(piece * wide, (piece + 1) * wide)
        total = jnp.dot(first, out_mine[:, columns], preferred_element_type=jnp.float32)
        total = total + jnp.dot(
            second, out_other[:, columns], preferred_element_type=jnp.float32
        )
        staged[:, columns] = total.astype(jnp.bfloat16)
        copies.append(
            pltpu.make_async_copy(staged.at[:, columns], result.at[:, columns], sems.at[piece])
        )
        copies[-1].start()
    for copy in copies:
        copy.wait()


def from_hbm(*arrays):
    return [pltpu.with_memory_space_constraint(array, pltpu.HBM) for array in arrays]


def exchanged(
    hidden_in, query_one, query_two, key_one, key_two, value_proj, lambdas, norm_gain, out_proj
):
    heads = lambdas.shape[0]
    groups = lax.axis_size("tp")
    down = across = 2
    parts = down * across
    rows, model = hidden_in.shape
    head_qk = query_one.shape[1] // heads
    width = heads * head_qk
    scale = 1.75 * head_qk ** (-0.5) * log2_e
    bf16 = jnp.bfloat16
    f32 = jnp.float32

    sp_index = lax.axis_index("sp")
    z = sp_index // parts
    y = (sp_index // across) % down
    x = sp_index % across
    place = jnp.stack([z, y, x]).astype(jnp.int32)

    def exchange(array, step):
        pairs = [(index, index ^ step) for index in range(heads * parts)]
        return lax.ppermute(array, "sp", pairs)

    swap_core = [(i, (i + 1) % groups) for i in range(groups)]
    turns = range(heads)

    block_rows = 2 * rows
    block = jax.ShapeDtypeStruct((block_rows, lanes), bf16)
    stripe = jax.ShapeDtypeStruct((rows, lanes), bf16)
    merged = jax.ShapeDtypeStruct((block_rows + rows, lanes), bf16)
    made = pl.pallas_call(
        functools.partial(project_kernel, heads),
        out_shape=[merged if turn == riding else block for turn in turns] + [stripe] * len(apart),
        in_specs=[in_smem()] + [in_hbm()] * 6,
        out_specs=[in_vmem()] * (heads + len(apart)),
        scratch_shapes=[
            pltpu.VMEM((rows, model), bf16),
            pltpu.VMEM((model, width), bf16),
            pltpu.VMEM((model, width), bf16),
            pltpu.VMEM((model, heads * lanes), bf16),
            pltpu.VMEM((model, width), bf16),
            pltpu.VMEM((model, width), bf16),
            pltpu.VMEM((heads, block_rows, lanes), bf16),
            pltpu.VMEM((heads, rows, lanes), bf16),
            pltpu.SemaphoreType.DMA((key_pieces, 6)),
        ],
        compiler_params=pltpu.CompilerParams(vmem_limit_bytes=20 << 20),
        cost_estimate=cost(2 * rows * model * 6 * width, 7 << 20),
        name="project",
    )(place, *from_hbm(hidden_in, key_one, key_two, value_proj, query_one, query_two))
    kv, queries = made[:heads], made[heads:]
    sent = [kv[0]] + [exchange(kv[turn], turn * parts) for turn in turns[1:]]
    own = [array[:block_rows] if turn == riding else array for turn, array in enumerate(sent)]
    own_queries = [queries[0]]
    for turn, array in zip(apart[1:], queries[1:]):
        own_queries.append(exchange(array, turn * parts))

    out_other = lax.ppermute(out_proj, "tp", swap_core)
    aside = [exchange(own[turn], 1) for turn in turns]
    below = [exchange(own[turn], across) for turn in turns]
    corner = [exchange(own[turn], 1 + across) for turn in turns]
    sides = (sent, aside, below, corner)
    last = heads // 2
    tokens = heads * rows
    early_blocks = [side[turn] for side in sides for turn in turns if turn != last]
    state = [
        jax.ShapeDtypeStruct((heads, rows, lanes), bf16),
        jax.ShapeDtypeStruct((parts * tokens, lanes), bf16),
        jax.ShapeDtypeStruct((lanes, parts * tokens), bf16),
        jax.ShapeDtypeStruct((heads, lanes, 2 * rows), f32),
        jax.ShapeDtypeStruct((heads, 8, 2 * rows), f32),
    ]
    state = pl.pallas_call(
        functools.partial(early_kernel, scale, heads, down, across),
        out_shape=state,
        in_specs=[in_smem()] + [in_vmem()] * (len(apart) + len(early_blocks)),
        out_specs=[in_vmem()] * 5,
        compiler_params=pltpu.CompilerParams(vmem_limit_bytes=28 << 20),
        cost_estimate=cost(3 * tokens * tokens * parts * lanes, 3 << 20),
        name="attend_early",
    )(place, *own_queries, *early_blocks)
    normed = pl.pallas_call(
        functools.partial(late_kernel, scale, heads, down, across),
        out_shape=[stripe] * heads,
        in_specs=[in_smem()] * 2 + [in_vmem()] * (1 + parts + 5),
        out_specs=[in_vmem()] * heads,
        scratch_shapes=[
            pltpu.VMEM((parts * rows, lanes), bf16),
            pltpu.VMEM((lanes, parts * rows), bf16),
            pltpu.VMEM((parts * tokens, lanes), bf16),
            pltpu.VMEM((lanes, parts * tokens), bf16),
            pltpu.VMEM((heads, rows, lanes), bf16),
            pltpu.VMEM((1, 2 * rows), f32),
            pltpu.VMEM((lanes, 2 * rows), f32),
            pltpu.VMEM((8, 2 * rows), f32),
            pltpu.VMEM((1, 2 * rows), f32),
        ],
        compiler_params=pltpu.CompilerParams(vmem_limit_bytes=28 << 20),
        cost_estimate=cost(tokens * tokens * parts * lanes, 3 << 20),
        name="attend_late",
    )(
        place,
        lambdas,
        norm_gain.reshape(1, lanes),
        *[side[last] for side in sides],
        *state,
    )

    back = [normed[0]]
    for turn in turns[1:]:
        back.append(exchange(normed[turn], turn * parts))
    back_other = [lax.ppermute(back[turn], "tp", swap_core) for turn in turns]
    return pl.pallas_call(
        functools.partial(project_out_kernel, heads),
        out_shape=jax.ShapeDtypeStruct((rows, model), bf16),
        in_specs=[in_smem()] + [in_vmem()] * (2 * heads + 2),
        out_specs=in_hbm(),
        scratch_shapes=[
            pltpu.VMEM((groups, heads, rows, lanes), bf16),
            pltpu.VMEM((rows, model), bf16),
            pltpu.SemaphoreType.DMA((4,)),
        ],
        compiler_params=pltpu.CompilerParams(vmem_limit_bytes=16 << 20),
        cost_estimate=cost(2 * rows * model * groups * heads * lanes, 6 << 20),
        name="project_out",
    )(place, *back, *back_other, out_proj, out_other)


def gathered(
    hidden_in, query_one, query_two, key_one, key_two, value_proj, lambdas, norm_gain, out_proj
):
    heads_dev = lambdas.shape[0]
    head_qk = query_one.shape[1] // heads_dev
    head_v = value_proj.shape[1] // heads_dev
    width_q = heads_dev * head_qk
    score_scale = 1.75 * head_qk ** (-0.5)
    joined = jnp.concatenate((query_one, query_two, key_one, key_two, value_proj), axis=1)
    projected = jnp.dot(hidden_in, joined, preferred_element_type=jnp.float32).astype(jnp.bfloat16)
    tok_rows = projected.shape[0]
    key_values = projected[:, 2 * width_q :]
    my_index = lax.axis_index("sp")
    positions = my_index * tok_rows + jnp.arange(tok_rows, dtype=jnp.int32)
    query_a = projected[:, :width_q].reshape(tok_rows, heads_dev, head_qk)
    query_b = projected[:, width_q : 2 * width_q].reshape(tok_rows, heads_dev, head_qk)
    last_pos = positions[tok_rows - 1]

    def one_map(queries, keys, value_rows, allowed, running_max, running_sum, accum):
        scores = (
            jnp.einsum("qhd,khd->hqk", queries, keys, preferred_element_type=jnp.float32)
            * score_scale
        )
        scores = jnp.where(allowed[None], scores, masked_score)
        new_max = jnp.maximum(running_max, jnp.max(scores, axis=-1))
        rescale = jnp.exp(running_max - new_max)
        weights = jnp.where(allowed[None], jnp.exp(scores - new_max[..., None]), 0.0)
        new_sum = running_sum * rescale + jnp.sum(weights, axis=-1)
        added = jnp.einsum(
            "hqk,khe->hqe",
            weights.astype(jnp.bfloat16),
            value_rows,
            preferred_element_type=jnp.float32,
        )
        return (new_max, new_sum, accum * rescale[..., None] + added)

    def absorb(state, kblock, kstart):
        block_rows = kblock.shape[0]
        k_pos = kstart + jnp.arange(block_rows, dtype=jnp.int32)
        allowed = k_pos[None, :] <= positions[:, None]
        keys_a = kblock[:, :width_q].reshape(block_rows, heads_dev, head_qk)
        keys_b = kblock[:, width_q : 2 * width_q].reshape(block_rows, heads_dev, head_qk)
        value_rows = kblock[:, 2 * width_q :].reshape(block_rows, heads_dev, head_v)
        first_map = one_map(query_a, keys_a, value_rows, allowed, *state[:3])
        second_map = one_map(query_b, keys_b, value_rows, allowed, *state[3:])
        return first_map + second_map

    start_max = jnp.full((heads_dev, tok_rows), masked_score, jnp.float32)
    start_sum = jnp.zeros((heads_dev, tok_rows), jnp.float32)
    start_acc = jnp.zeros((heads_dev, tok_rows, head_v), jnp.float32)
    state = (start_max, start_sum, start_acc, start_max, start_sum, start_acc)
    kv_piece = lax.all_gather(key_values, "sp", axis=0, tiled=True)
    piece_rows = kv_piece.shape[0]
    block_rows = math.gcd(piece_rows, 512)
    block_count = piece_rows // block_rows
    stacked = kv_piece.reshape(block_count, block_rows, kv_piece.shape[1])

    def absorb_step(carried, blocks_in):
        kblock, block_index = blocks_in
        kstart = block_index * block_rows
        renewed = lax.cond(
            kstart <= last_pos,
            lambda inner: absorb(inner, kblock, kstart),
            lambda inner: inner,
            carried,
        )
        return (renewed, None)

    state, _ = lax.scan(absorb_step, state, (stacked, jnp.arange(block_count, dtype=jnp.int32)))
    out_a = state[2] / state[1][..., None]
    out_b = state[5] / state[4][..., None]
    mixed_out = out_a - lambdas[:, None, None] * out_b
    scale_rows = lax.rsqrt(jnp.mean(mixed_out * mixed_out, axis=-1, keepdims=True) + epsilon)
    normed = (mixed_out * scale_rows * norm_gain).astype(jnp.bfloat16)
    normed_all = jnp.transpose(normed, (1, 0, 2)).reshape(tok_rows, heads_dev * head_v)
    partial_value = jnp.dot(normed_all, out_proj, preferred_element_type=jnp.float32)
    return lax.psum(partial_value.astype(jnp.bfloat16), "tp")


def shards(*args):
    hidden_in, query_one, value_proj, lambdas = args[0], args[1], args[5], args[6]
    heads = lambdas.shape[0]
    groups, length = lax.axis_size("tp"), lax.axis_size("sp")
    fits = (
        groups == 2
        and heads == 4
        and length == 4 * heads
        and query_one.shape[1] == heads * (lanes // 2)
        and value_proj.shape[1] == heads * lanes
        and hidden_in.shape[0] % lanes == 0
        and hidden_in.shape[0] <= 512
    )
    if not fits:
        return gathered(*args)
    return exchanged(*args)


def solution(mesh):
    placed = (
        P("sp", None),
        P(None, "tp"),
        P(None, "tp"),
        P(None, "tp"),
        P(None, "tp"),
        P(None, "tp"),
        P("tp"),
        P(),
        P("tp", None),
    )
    return jax.shard_map(
        shards, mesh=mesh, in_specs=placed, out_specs=P("sp", None), check_vma=False
    )
```
